128 devices in a mesh: kv: 16 (over z, y), tp: 8 (over x, core).
Axes of the slice: x: 4, y: 4, z: 4, core: 2. Of those that a mesh axis runs over, the one named last changes fastest.
Arguments:
- block_in: bfloat16 [128, 4096], P(None, ('kv', 'tp')), may hold values from -30 to 30
- before_gain: bfloat16 [4096], P('kv'), may hold values from 0.099609375 to 1.8984375
- before_gate: bfloat16 [4096, 11264], P('kv', 'tp'), may hold values from -0.09375 to 0.09375
- before_up: bfloat16 [4096, 11264], P('kv', 'tp'), may hold values from -0.09375 to 0.09375
- before_down: bfloat16 [11264, 4096], P('tp', 'kv'), may hold values from -0.0546875 to 0.0546875
- mix_gain: bfloat16 [4096], P('kv'), may hold values from 0.099609375 to 1.8984375
- input_gate: bfloat16 [4096, 8192], P('kv', 'tp'), may hold values from -0.09375 to 0.09375
- input_value: bfloat16 [4096, 8192], P('kv', 'tp'), may hold values from -0.09375 to 0.09375
- input_write: bfloat16 [4096, 2048], P('kv', 'tp'), may hold values from -0.09375 to 0.09375
- input_read: bfloat16 [4096, 2048], P('kv', 'tp'), may hold values from -0.09375 to 0.09375
- input_step: bfloat16 [4096, 128], P('kv', 'tp'), may hold values from -0.09375 to 0.09375
- step_bias: float32 [128], P('tp'), may hold values from -3 to 0
- decay_log: float32 [128], P('tp'), may hold values from -1 to 1.4
- skip_gain: float32 [128], P('tp'), may hold values from 0.5 to 2
- value_taps: bfloat16 [4, 8192], P(None, 'tp'), may hold values from -3 to 3
- write_taps: bfloat16 [4, 2048], P(None, 'tp'), may hold values from -3 to 3
- read_taps: bfloat16 [4, 2048], P(None, 'tp'), may hold values from -3 to 3
- value_window: bfloat16 [128, 3, 8192], P('kv', None, 'tp'), may hold values from -6 to 6
- write_window: bfloat16 [128, 3, 2048], P('kv', None, 'tp'), may hold values from -6 to 6
- read_window: bfloat16 [128, 3, 2048], P('kv', None, 'tp'), may hold values from -6 to 6
- scan_state: float32 [128, 128, 64, 128], P('kv', 'tp'), may hold values from -2 to 2
- group_gain: bfloat16 [8192], P('tp'), may hold values from 0.099609375 to 1.8984375
- mixer_out: bfloat16 [8192, 4096], P('tp', 'kv'), may hold values from -0.0625 to 0.0625
- after_gain: bfloat16 [4096], P('kv'), may hold values from 0.099609375 to 1.8984375
- after_gate: bfloat16 [4096, 11264], P('kv', 'tp'), may hold values from -0.09375 to 0.09375
- after_up: bfloat16 [4096, 11264], P('kv', 'tp'), may hold values from -0.09375 to 0.09375
- after_down: bfloat16 [11264, 4096], P('tp', 'kv'), may hold values from -0.0546875 to 0.0546875
Outputs:
- block_out: bfloat16 [128, 4096], P(None, ('kv', 'tp'))
- state_next: float32 [128, 128, 64, 128], P('kv', 'tp')
- value_next: bfloat16 [128, 3, 8192], P('kv', None, 'tp')
- write_next: bfloat16 [128, 3, 2048], P('kv', None, 'tp')
- read_next: bfloat16 [128, 3, 2048], P('kv', None, 'tp')
The draws below stay inside these ranges and needn't reach their ends.
All inputs are finite; a program needn't handle non-finite values.
Results may differ from the reference program's by a relative error of at most 0.0085.
Values may be sent and summed in bfloat16 or wider, within the bound.
A program may use at most 64 MiB of HBM per device.

```python
import math
import jax
import jax.numpy as jnp
from jax import lax

D = 4096
FF = 11264
INNER = 8192
HEAD_DIM = 64
HEADS = 128
GROUPS = 16
STATE = 128
CONV = 4
BATCH = 128
N_KV = 16
N_TP = 8


def draw_block_in(key, part):
    base_key = jax.random.fold_in(key, 11)
    first_key, second_key = jax.random.split(base_key, 2)
    columns = jnp.arange(D, dtype=jnp.int32)
    column_block = D // (N_KV * N_TP)
    tp_place = (columns // column_block % N_TP).astype(jnp.float32)
    column_scale = jnp.exp(1.6 * columns.astype(jnp.float32) / D + 0.7 * tp_place / max(N_TP - 1, 1))
    row_scale = jnp.exp(jax.random.uniform(second_key, (BATCH, 1), jnp.float32, 0.0, 1.1))
    values = jnp.clip(jax.random.normal(first_key, (BATCH, D), jnp.float32), -4.0, 4.0)
    return (0.25 * values * row_scale * column_scale[None, :]).astype(jnp.bfloat16)


def shard_levels(own_key, extent, shards, low, largest):
    loudness = 1.0
    for position, parts in shards:
        heights = jax.random.uniform(jax.random.fold_in(jax.random.fold_in(own_key, 6), position), (parts,), jnp.float32, low / len(shards), largest / len(shards))
        loudness = loudness * jnp.repeat(jnp.exp(heights), extent[position] // parts).reshape((-1,) + (1,) * (len(extent) - 1 - position))
    return loudness


def centred(stream_key, extent, spread, reach, shards=(), kind=jnp.bfloat16):
    entries = spread * jax.random.normal(stream_key, extent, jnp.float32)
    if shards:
        entries = entries * shard_levels(stream_key, extent, shards, -0.22, 0.18)
    return jnp.clip(entries, -reach, reach).astype(kind)


def setup_inputs(seed: int = 0) -> dict:
    arg_keys = jax.random.split(jax.random.key(seed), 28)
    block_in = draw_block_in(jax.random.fold_in(arg_keys[27], 71), 0)
    before_gain = jnp.clip(1.0 + 0.18 * jax.random.normal(arg_keys[1], (D,), jnp.float32), 0.099609375, 1.8984375).astype(jnp.bfloat16)
    before_gate = centred(arg_keys[2], (D, FF), D ** -0.5, 0.09375, ((0, 16), (1, 8)))
    before_up = centred(arg_keys[3], (D, FF), D ** -0.5, 0.09375, ((0, 16), (1, 8)))
    before_down = centred(arg_keys[4], (FF, D), FF ** -0.5, 0.0546875, ((0, 8), (1, 16)))
    mix_gain = jnp.clip(1.0 + 0.18 * jax.random.normal(arg_keys[5], (D,), jnp.float32), 0.099609375, 1.8984375).astype(jnp.bfloat16)
    input_gate = centred(arg_keys[6], (D, INNER), D ** -0.5, 0.09375, ((0, 16), (1, 8)))
    input_value = centred(arg_keys[7], (D, INNER), D ** -0.5, 0.09375, ((0, 16), (1, 8)))
    input_write = centred(arg_keys[8], (D, GROUPS * STATE), D ** -0.5, 0.09375, ((0, 16), (1, 8)))
    input_read = centred(arg_keys[9], (D, GROUPS * STATE), D ** -0.5, 0.09375, ((0, 16), (1, 8)))
    input_step = centred(arg_keys[10], (D, HEADS), D ** -0.5, 0.09375, ((0, 16), (1, 8)))
    step_bias = jnp.clip(-3.0 + 3.0 * jax.random.uniform(arg_keys[11], (HEADS,), jnp.float32) ** shard_levels(arg_keys[11], (HEADS,), ((0, 8),), -0.2, 0.2), -3.0, 0.0)
    decay_log = jnp.clip(-1.0 + 2.4 * jax.random.uniform(arg_keys[12], (HEADS,), jnp.float32) ** shard_levels(arg_keys[12], (HEADS,), ((0, 8),), -0.2, 0.2), -1.0, 1.4)
    skip_gain = jnp.clip(jnp.exp(math.log(2.0) - 1.3862944 * jax.random.uniform(arg_keys[13], (HEADS,), jnp.float32) ** shard_levels(arg_keys[13], (HEADS,), ((0, 8),), -0.2, 0.2)), 0.5, 2.0)
    value_taps = centred(arg_keys[14], (CONV, INNER), CONV ** -0.5, 3.0, ((1, 8),))
    write_taps = centred(arg_keys[15], (CONV, GROUPS * STATE), CONV ** -0.5, 3.0, ((1, 8),))
    read_taps = centred(arg_keys[16], (CONV, GROUPS * STATE), CONV ** -0.5, 3.0, ((1, 8),))
    value_window = centred(arg_keys[17], (BATCH, CONV - 1, INNER), 1.0, 6.0, ((0, 16), (2, 8)))
    write_window = centred(arg_keys[18], (BATCH, CONV - 1, GROUPS * STATE), 1.0, 6.0, ((0, 16), (2, 8)))
    read_window = centred(arg_keys[19], (BATCH, CONV - 1, GROUPS * STATE), 1.0, 6.0, ((0, 16), (2, 8)))
    scan_state = centred(arg_keys[20], (BATCH, HEADS, HEAD_DIM, STATE), 0.3, 2.0, ((0, 16), (1, 8)), jnp.float32)
    group_gain = jnp.clip(1.0 + 0.18 * jax.random.normal(arg_keys[21], (INNER,), jnp.float32), 0.099609375, 1.8984375).astype(jnp.bfloat16)
    mixer_out = centred(arg_keys[22], (INNER, D), INNER ** -0.5, 0.0625, ((0, 8), (1, 16)))
    after_gain = jnp.clip(1.0 + 0.18 * jax.random.normal(arg_keys[23], (D,), jnp.float32), 0.099609375, 1.8984375).astype(jnp.bfloat16)
    after_gate = centred(arg_keys[24], (D, FF), D ** -0.5, 0.09375, ((0, 16), (1, 8)))
    after_up = centred(arg_keys[25], (D, FF), D ** -0.5, 0.09375, ((0, 16), (1, 8)))
    after_down = centred(arg_keys[26], (FF, D), FF ** -0.5, 0.0546875, ((0, 8), (1, 16)))
    return dict(block_in=block_in, before_gain=before_gain, before_gate=before_gate, before_up=before_up, before_down=before_down, mix_gain=mix_gain, input_gate=input_gate, input_value=input_value, input_write=input_write, input_read=input_read, input_step=input_step, step_bias=step_bias, decay_log=decay_log, skip_gain=skip_gain, value_taps=value_taps, write_taps=write_taps, read_taps=read_taps, value_window=value_window, write_window=write_window, read_window=read_window, scan_state=scan_state, group_gain=group_gain, mixer_out=mixer_out, after_gain=after_gain, after_gate=after_gate, after_up=after_up, after_down=after_down)


EPS = 1e-06

def half_channel(current, gain_vec, gate_weight, up_weight, down_weight):
    widened = current.astype(jnp.float32)
    row_scale = lax.rsqrt(lax.optimization_barrier(jnp.mean(widened * widened, axis=1, keepdims=True)) + EPS)
    lifted = (widened * gain_vec.astype(jnp.float32)).astype(jnp.bfloat16)
    gate_sum = jnp.dot(lifted, gate_weight, preferred_element_type=jnp.float32) * row_scale
    up_sum = jnp.dot(lifted, up_weight, preferred_element_type=jnp.float32) * row_scale
    hidden = (jax.nn.silu(gate_sum) * up_sum).astype(jnp.bfloat16)
    down_sum = jnp.dot(hidden, down_weight, preferred_element_type=jnp.float32)
    return (widened + 0.5 * down_sum).astype(jnp.bfloat16)

def short_conv(window_state, fresh, taps):
    window = jnp.concatenate([window_state, fresh[:, None, :]], axis=1)
    conv_sum = lax.optimization_barrier(jnp.sum(window.astype(jnp.float32) * taps.astype(jnp.float32)[None], axis=1))
    return (jax.nn.silu(conv_sum), window[:, 1:])

def spread_groups(vectors, heads):
    count = vectors.shape[0]
    groups = vectors.shape[1] // STATE
    shaped = vectors.reshape(count, groups, 1, STATE)
    return jnp.broadcast_to(shaped, (count, groups, heads // groups, STATE)).reshape(count, heads, STATE)

def state_update(gate_rows, value_conv, write_conv, read_conv, step_raw, step_bias, decay_log, skip_gain, scan_state):
    count = value_conv.shape[0]
    heads = step_bias.shape[0]
    step_size = jax.nn.softplus(step_raw + step_bias[None, :])
    decay = jnp.exp(-step_size * jnp.exp(decay_log)[None, :])
    value_heads = value_conv.reshape(count, heads, HEAD_DIM)
    write_heads = spread_groups(write_conv, heads)
    read_heads = spread_groups(read_conv, heads)
    state_next = decay[:, :, None, None] * scan_state + (step_size[:, :, None] * value_heads)[:, :, :, None] * write_heads[:, :, None, :]
    readout = lax.optimization_barrier(jnp.sum(state_next * read_heads[:, :, None, :], axis=3)) + skip_gain[None, :, None] * value_heads
    gated = readout.reshape(count, heads * HEAD_DIM) * jax.nn.silu(gate_rows.astype(jnp.float32))
    groups = write_conv.shape[1] // STATE
    grouped = gated.reshape(count, groups, heads * HEAD_DIM // groups)
    grouped = grouped * lax.rsqrt(lax.optimization_barrier(jnp.mean(grouped * grouped, axis=2, keepdims=True)) + EPS)
    return (grouped.reshape(count, heads * HEAD_DIM), state_next)

def reference(block_in, before_gain, before_gate, before_up, before_down, mix_gain, input_gate, input_value, input_write, input_read, input_step, step_bias, decay_log, skip_gain, value_taps, write_taps, read_taps, value_window, write_window, read_window, scan_state, group_gain, mixer_out, after_gain, after_gate, after_up, after_down):
    first_out = half_channel(block_in, before_gain, before_gate, before_up, before_down)
    widened = first_out.astype(jnp.float32)
    mix_scale = lax.rsqrt(lax.optimization_barrier(jnp.mean(widened * widened, axis=1, keepdims=True)) + EPS)
    lifted = (widened * mix_gain.astype(jnp.float32)).astype(jnp.bfloat16)
    gate_rows = (jnp.dot(lifted, input_gate, preferred_element_type=jnp.float32) * mix_scale).astype(jnp.bfloat16)
    value_fresh = (jnp.dot(lifted, input_value, preferred_element_type=jnp.float32) * mix_scale).astype(jnp.bfloat16)
    write_fresh = (jnp.dot(lifted, input_write, preferred_element_type=jnp.float32) * mix_scale).astype(jnp.bfloat16)
    read_fresh = (jnp.dot(lifted, input_read, preferred_element_type=jnp.float32) * mix_scale).astype(jnp.bfloat16)
    step_raw = jnp.dot(lifted, input_step, preferred_element_type=jnp.float32) * mix_scale
    value_conv, value_next = short_conv(value_window, value_fresh, value_taps)
    write_conv, write_next = short_conv(write_window, write_fresh, write_taps)
    read_conv, read_next = short_conv(read_window, read_fresh, read_taps)
    normed, state_next = state_update(gate_rows, value_conv, write_conv, read_conv, step_raw, step_bias, decay_log, skip_gain, scan_state)
    mixer_rows = (normed * group_gain.astype(jnp.float32)[None, :]).astype(jnp.bfloat16)
    middle = (widened + jnp.dot(mixer_rows, mixer_out, preferred_element_type=jnp.float32)).astype(jnp.bfloat16)
    block_out = half_channel(middle, after_gain, after_gate, after_up, after_down)
    return (block_out, state_next, value_next, write_next, read_next)
```

```python
import jax
import jax.numpy as jnp
from jax import lax
from jax.experimental import pallas as pl
from jax.experimental.pallas import tpu as pltpu
from jax.sharding import PartitionSpec as P

D = 4096
HEAD_DIM = 64
STATE = 128
EPS = 1e-06

KV = 16
TP = 8
ROWS = 128
FEAT = 256
HID = 1408
INNER = 1024
HEADS = 16
CHUNKS = ((0, 768), (768, 640))
EXTRA = 128
GROUP = 512

F32 = jnp.float32
BF16 = jnp.bfloat16
MESH = pl.DeviceIdType.MESH


def silu(v):
    return v / (1.0 + jnp.exp(-v))


def dot(a, b):
    return jnp.dot(a, b, preferred_element_type=F32)


class Exchange:
    def __init__(self):
        self.kv = lax.axis_index("kv")
        self.tp = lax.axis_index("tp")
        self.z = self.kv // 4
        self.y = self.kv % 4
        self.sent = []

    def kv_peer(self, d):
        return ((self.z + d // 4) % 4) * 4 + (self.y + d % 4) % 4

    def tp_peer(self, d):
        return (self.tp + d) % 8

    def barrier(self):
        bar = pltpu.get_barrier_semaphore()

        def greet_kv(d, c):
            pl.semaphore_signal(bar, inc=1, device_id=(self.kv_peer(d), self.tp), device_id_type=MESH)
            return c

        def greet_tp(d, c):
            pl.semaphore_signal(bar, inc=1, device_id=(self.kv, self.tp_peer(d)), device_id_type=MESH)
            return c

        lax.fori_loop(1, TP, greet_tp, 0)
        lax.fori_loop(1, KV, greet_kv, 0)
        pl.semaphore_wait(bar, KV + TP - 2)

    def _run(self, count, copy_of):
        def step(d, c):
            copy_of(d).start()
            return c

        lax.fori_loop(1, count, step, 0)

    def scatter(self, axis, src, dst, sems):
        def copy_of(d):
            if axis == "kv":
                to = self.kv_peer(d)
                where = (to, self.tp)
            else:
                to = self.tp_peer(d)
                where = (self.kv, to)
            return pltpu.make_async_remote_copy(
                src.at[to], dst.at[d - 1], sems.at[0], sems.at[1], device_id=where, device_id_type=MESH
            )

        count = KV if axis == "kv" else TP
        self._run(count, copy_of)
        self.sent.append((dst, sems))

    def spread(self, axis, buf, sems):
        me = self.kv if axis == "kv" else self.tp

        def copy_of(d):
            where = (self.kv_peer(d), self.tp) if axis == "kv" else (self.kv, self.tp_peer(d))
            return pltpu.make_async_remote_copy(
                buf.at[me], buf.at[me], sems.at[0], sems.at[1], device_id=where, device_id_type=MESH
            )

        count = KV if axis == "kv" else TP
        self._run(count, copy_of)
        self.sent.append((buf.at[pl.ds(0, count - 1)], sems))

    def arrived(self, dst, sems):
        pltpu.make_async_copy(dst, dst, sems.at[1]).wait()

    def drain(self):
        for dst, sems in self.sent:
            pltpu.make_async_copy(dst, dst, sems.at[0]).wait()


def as_blocks(ref, lanes, value):
    lo, size = lanes
    ref[:, :, lo : lo + size] = value.reshape(KV, 8, size).astype(BF16)


def summed(recv, own, me):
    total = own[me].astype(F32)
    for d in range(KV - 1):
        total = total + recv[d].astype(F32)
    return total


def split_high(value):
    high = value.astype(BF16).astype(F32)
    return high, value - high


def lift(cur, gain_ref):
    wide = cur.astype(F32)
    squares = jnp.sum(wide * wide, axis=1, keepdims=True)
    lifted = (wide * gain_ref[...].reshape(1, FEAT).astype(F32)).astype(BF16)
    return lifted, squares


def full_rows(buf):
    blocks = buf[...]
    return blocks.astype(F32).reshape(ROWS, blocks.shape[2]).astype(BF16)


def half_channel(ex, cur, which, vmem, loaded, send, recv, hid, sem):
    gain, gate, up, down = (which + end for end in ("_gain", "_gate", "_up", "_down"))
    gate_w, up_w, down_w = vmem[gate], vmem[up], vmem[down]
    loaded(gain)
    lifted, squares = lift(cur, vmem[gain])
    lane = lax.broadcasted_iota(jnp.int32, (ROWS, EXTRA), 1)
    high, low = split_high(squares)
    loaded(gate, up)
    for i, (lo, size) in enumerate(CHUNKS):
        as_blocks(send[i], (0, size), dot(lifted, gate_w[:, lo : lo + size]))
        as_blocks(send[i], (size, size), dot(lifted, up_w[:, lo : lo + size]))
        if i == 0:
            as_blocks(send[i], (2 * size, EXTRA), jnp.where(lane < 64, high, low))
        ex.scatter("kv", send[i], recv[i], sem.at[i])
    scale = None
    for i, (lo, size) in enumerate(CHUNKS):
        ex.arrived(recv[i], sem.at[i])
        total = summed(recv[i], send[i], ex.kv)
        if i == 0:
            t = total[:, 2 * size : 2 * size + 1] + total[:, 2 * size + 64 : 2 * size + 65]
            scale = lax.rsqrt(t / D + EPS)
        hidden = silu(total[:, :size] * scale) * (total[:, size : 2 * size] * scale)
        hid[i][ex.kv] = hidden.astype(BF16)
        ex.spread("kv", hid[i], sem.at[2 + i])
    loaded(down)
    part = None
    for i, (lo, size) in enumerate(CHUNKS):
        ex.arrived(hid[i].at[pl.ds(0, KV - 1)], sem.at[2 + i])
        p = dot(full_rows(hid[i]), down_w[lo : lo + size, :])
        part = p if part is None else part + p
    return part


def row_exchange(ex, part, cur_ref, factor, f32_buf, send, recv, out, sem):
    f32_buf[...] = part
    send[...] = part.reshape(TP, 16, FEAT).astype(BF16)
    ex.scatter("tp", send, recv, sem.at[0])
    mine = pl.ds(pl.multiple_of(ex.tp * 16, 16), 16)
    total = f32_buf[mine, :]
    ex.arrived(recv, sem.at[0])
    for d in range(TP - 1):
        total = total + recv[d].astype(F32)
    out[ex.tp] = (cur_ref[ex.tp].astype(F32) + factor * total).astype(BF16)
    ex.spread("tp", out, sem.at[1])
    ex.arrived(out.at[pl.ds(0, TP - 1)], sem.at[1])
    return out[...].reshape(ROWS, FEAT)


NAMES = (
    "block_in", "before_gain", "before_gate", "before_up", "before_down", "mix_gain", "input_gate",
    "input_value", "input_write", "input_read", "input_step", "step_bias", "decay_log", "skip_gain",
    "value_taps", "write_taps", "read_taps", "value_window", "write_window", "read_window", "scan_state",
    "group_gain", "mixer_out", "after_gain", "after_gate", "after_up", "after_down",
)


def kernel(
    *refs,
):
    count = len(NAMES)
    hbm = dict(zip(NAMES, refs[:count]))
    block_out, state_out, value_next, write_next, read_next = refs[count : count + 5]
    vmem = dict(zip(NAMES, refs[count + 5 : 2 * count + 5]))
    load_sem, *rest = refs[2 * count + 5 :]
    (
        packed, cur0, cur1, cur2, f32_buf,
        a_send0, a_send1, a_recv0, a_recv1, a_hid0, a_hid1,
        m_send0, m_send1, m_recv0, m_recv1, m_hid0, m_hid1,
        b_send0, b_send1, b_recv0, b_recv1, b_hid0, b_hid1,
        t1_send, t1_recv, t2_send, t2_recv, t3_own, t3_send, t3_recv,
        sem_in, sem_a, sem_m, sem_b, sem_t1, sem_t2, sem_t3,
    ) = rest
    ex = Exchange()
    loads = {n: pltpu.make_async_copy(hbm[n], vmem[n], load_sem.at[i]) for i, n in enumerate(NAMES) if n != "block_in"}
    mine = pltpu.make_async_copy(hbm["block_in"], packed.at[ex.tp], load_sem.at[0])
    mine.start()
    for copy in loads.values():
        copy.start()

    def loaded(*names):
        for n in names:
            loads[n].wait()

    ex.barrier()
    mine.wait()
    ex.spread("tp", packed, sem_in)
    ex.arrived(packed.at[pl.ds(0, TP - 1)], sem_in)
    cur = jnp.transpose(packed[...].astype(F32).reshape(FEAT, ROWS)).astype(BF16)
    cur0[...] = cur.reshape(TP, 16, FEAT)

    part = half_channel(
        ex, cur, "before", vmem, loaded,
        (a_send0, a_send1), (a_recv0, a_recv1), (a_hid0, a_hid1), sem_a,
    )
    cur = row_exchange(ex, part, cur0, 0.5, f32_buf, t1_send, t1_recv, cur1, sem_t1)

    loaded("mix_gain", "input_gate", "input_value", "input_write", "input_read", "input_step")
    lifted, squares = lift(cur, vmem["mix_gain"])
    m_send, m_recv, m_hid = (m_send0, m_send1), (m_recv0, m_recv1), (m_hid0, m_hid1)
    for g in range(2):
        wide, narrow = slice(GROUP * g, GROUP * g + GROUP), slice(STATE * g, STATE * g + STATE)
        as_blocks(m_send[g], (0, GROUP), dot(lifted, vmem["input_gate"][:, wide]))
        as_blocks(m_send[g], (GROUP, GROUP), dot(lifted, vmem["input_value"][:, wide]))
        as_blocks(m_send[g], (2 * GROUP, STATE), dot(lifted, vmem["input_write"][:, narrow]))
        as_blocks(m_send[g], (2 * GROUP + STATE, STATE), dot(lifted, vmem["input_read"][:, narrow]))
        if g == 0:
            place = lax.broadcasted_iota(jnp.int32, (EXTRA, HEADS), 0)
            head = lax.broadcasted_iota(jnp.int32, (EXTRA, HEADS), 1)
            spots = jnp.where((place % HEADS == head) & (place < 2 * HEADS), 1.0, 0.0).astype(BF16)
            step_w = dot(spots, vmem["input_step"][...]).astype(BF16)
            step = lax.dot_general(lifted, step_w, (((1,), (1,)), ((), ())), preferred_element_type=F32)
            lane = lax.broadcasted_iota(jnp.int32, (ROWS, EXTRA), 1)
            value = jnp.where(lane < 2 * HEADS, step, squares)
            high, low = split_high(value)
            lows = ((lane >= HEADS) & (lane < 2 * HEADS)) | (lane >= 80)
            as_blocks(m_send[g], (2 * GROUP + 2 * STATE, EXTRA), jnp.where(lows, low, high))
        ex.scatter("kv", m_send[g], m_recv[g], sem_m.at[g])

    scale = None
    for g in range(2):
        wide, narrow = slice(GROUP * g, GROUP * g + GROUP), slice(STATE * g, STATE * g + STATE)
        if g == 0:
            loaded("step_bias", "decay_log", "skip_gain", "group_gain")
            loaded(*(a + b for a in ("value", "write", "read") for b in ("_taps", "_window")))
        ex.arrived(m_recv[g], sem_m.at[g])
        total = summed(m_recv[g], m_send[g], ex.kv)
        if g == 0:
            tile = total[:, 2 * GROUP + 2 * STATE :]
            scale = lax.rsqrt((tile[:, 32:33] + tile[:, 80:81]) / D + EPS)
            raw = (tile + pltpu.roll(tile, EXTRA - HEADS, 1))[:, :HEADS] * scale
            raw = raw + vmem["step_bias"][...].reshape(1, HEADS)
            step_size = jnp.maximum(raw, 0.0) + jnp.log1p(jnp.exp(-jnp.abs(raw)))
            decay = jnp.exp(-step_size * jnp.exp(vmem["decay_log"][...].reshape(1, HEADS)))
            skip = jnp.broadcast_to(vmem["skip_gain"][...].reshape(1, HEADS), (8, HEADS))
            heads = jnp.concatenate([step_size, decay, skip], axis=0)
            of = lax.broadcasted_iota(jnp.int32, (HEADS, INNER), 1) // HEAD_DIM
            row = lax.broadcasted_iota(jnp.int32, (HEADS, INNER), 0)
            expand = jnp.where(of == row, 1.0, 0.0)
            heads = jnp.dot(heads, expand, preferred_element_type=F32, precision=lax.Precision.HIGHEST)

        def conv(col, size, next_ref, kind, lanes):
            fresh = (total[:, col : col + size] * scale).astype(BF16)
            window = [vmem[kind + "_window"][i, :, lanes] for i in range(3)] + [fresh]
            k = vmem[kind + "_taps"][:, lanes].astype(F32)
            acc = None
            for i in range(4):
                if i:
                    next_ref[i - 1, :, lanes] = window[i]
                term = window[i].astype(F32) * k[i : i + 1]
                acc = term if acc is None else acc + term
            return silu(acc)

        gate_rows = (total[:, :GROUP] * scale).astype(BF16).astype(F32)
        value = conv(GROUP, GROUP, value_next, "value", wide)
        write = conv(2 * GROUP, STATE, write_next, "write", narrow)
        read = conv(2 * GROUP + STATE, STATE, read_next, "read", narrow)
        step_x = heads[0:8, wide] * value
        across = jnp.transpose(jnp.concatenate([step_x, heads[8:16, wide]], axis=0))
        if g == 0:
            loaded("scan_state")
        readout = jnp.zeros((GROUP, 128), F32)
        column = lax.broadcasted_iota(jnp.int32, (STATE, 128), 1)
        read_across = jnp.transpose(jnp.concatenate([read] * 16, axis=0))
        for r in range(8):
            old = vmem["scan_state"][r, 8 * g : 8 * g + 8].reshape(GROUP, STATE)
            new = across[:, 8 + r : 9 + r] * old + across[:, r : r + 1] * write[r : r + 1]
            state_out[r, 8 * g : 8 * g + 8] = new.reshape(8, HEAD_DIM, STATE)
            one = jnp.where(column == r, read_across, 0.0).astype(BF16)
            readout = readout + dot(new.astype(BF16), one)
        readout = jnp.transpose(readout)[0:8]
        readout = readout + heads[16:24, wide] * value
        gated = readout * silu(gate_rows)
        mean = jnp.sum(gated * gated, axis=1, keepdims=True) / GROUP
        normed = gated * lax.rsqrt(mean + EPS)
        gain = vmem["group_gain"][...].reshape(1, INNER)[:, wide].astype(F32)
        m_hid[g][ex.kv] = (normed * gain).astype(BF16)
        ex.spread("kv", m_hid[g], sem_m.at[2 + g])
    loaded("mixer_out")
    part = None
    for g in range(2):
        ex.arrived(m_hid[g].at[pl.ds(0, KV - 1)], sem_m.at[2 + g])
        p = dot(full_rows(m_hid[g]), vmem["mixer_out"][GROUP * g : GROUP * g + GROUP, :])
        part = p if part is None else part + p
    cur = row_exchange(ex, part, cur1, 1.0, f32_buf, t2_send, t2_recv, cur2, sem_t2)

    part = half_channel(
        ex, cur, "after", vmem, loaded,
        (b_send0, b_send1), (b_recv0, b_recv1), (b_hid0, b_hid1), sem_b,
    )
    columns = jnp.transpose(part).reshape(TP, 32, ROWS)
    t3_own[...] = columns
    t3_send[...] = columns.astype(BF16)
    ex.scatter("tp", t3_send, t3_recv, sem_t3)
    total = t3_own[ex.tp]
    t3_own[...] = jnp.transpose(cur.astype(F32)).reshape(TP, 32, ROWS)
    ex.arrived(t3_recv, sem_t3)
    for d in range(TP - 1):
        total = total + t3_recv[d].astype(F32)
    block_out[...] = (t3_own[ex.tp] + 0.5 * total).astype(BF16)
    ex.drain()


def store(*refs):
    srcs, dsts, sem = refs[: (len(refs) - 1) // 2], refs[(len(refs) - 1) // 2 : -1], refs[-1]
    copies = [pltpu.make_async_copy(s, d, sem.at[i]) for i, (s, d) in enumerate(zip(srcs, dsts))]
    for copy in copies:
        copy.start()
    for copy in copies:
        copy.wait()


def local(*args):
    named = dict(zip(NAMES, args))
    named["block_in"] = named["block_in"].T
    named["input_step"] = named["input_step"].T
    for kind in ("value", "write", "read"):
        named[kind + "_window"] = named[kind + "_window"].transpose(1, 0, 2)
    operands = [pltpu.with_memory_space_constraint(named[n], pltpu.HBM) for n in NAMES]
    vmem = pl.BlockSpec(memory_space=pltpu.VMEM)
    hbm = pl.BlockSpec(memory_space=pltpu.HBM)

    def v(*shape, dtype=BF16):
        return pltpu.VMEM(shape, dtype)

    def kv_buffers(widths, hidden):
        return (
            [v(KV, 8, w) for w in widths] + [v(KV - 1, 8, w) for w in widths] + [v(KV, 8, h) for h in hidden]
        )

    channel = kv_buffers([2 * s + (EXTRA if i == 0 else 0) for i, (_, s) in enumerate(CHUNKS)], [s for _, s in CHUNKS])
    mixer = kv_buffers([2 * GROUP + 2 * STATE + EXTRA, 2 * GROUP + 2 * STATE], [GROUP, GROUP])
    sems = pltpu.SemaphoreType.DMA
    shapes = (
        jax.ShapeDtypeStruct((32, ROWS), BF16),
        jax.ShapeDtypeStruct(named["scan_state"].shape, F32),
        jax.ShapeDtypeStruct((3, 8, INNER), BF16),
        jax.ShapeDtypeStruct((3, 8, 256), BF16),
        jax.ShapeDtypeStruct((3, 8, 256), BF16),
    )
    results = pl.pallas_call(
        kernel,
        out_shape=shapes,
        in_specs=[hbm] * len(operands),
        out_specs=(vmem,) * 5,
        scratch_shapes=[
            *[v(*a.shape, dtype=a.dtype) for a in operands],
            sems((len(NAMES),)),
            v(TP, 32, 128), v(TP, 16, FEAT), v(TP, 16, FEAT), v(TP, 16, FEAT), v(ROWS, FEAT, dtype=F32),
            *channel, *mixer, *channel,
            v(TP, 16, FEAT), v(TP - 1, 16, FEAT), v(TP, 16, FEAT), v(TP - 1, 16, FEAT),
            v(TP, 32, 128, dtype=F32), v(TP, 32, 128), v(TP - 1, 32, 128),
            sems((2,)), sems((4, 2)), sems((4, 2)), sems((4, 2)), sems((2, 2)), sems((2, 2)), sems((2,)),
        ],
        compiler_params=pltpu.CompilerParams(
            collective_id=0, has_side_effects=True, vmem_limit_bytes=40 * 1024 * 1024
        ),
        name="layer",
    )(*operands)
    block_out, state_next, *windows = pl.pallas_call(
        store,
        out_shape=shapes,
        in_specs=[vmem] * 5,
        out_specs=(hbm,) * 5,
        scratch_shapes=[sems((5,))],
        compiler_params=pltpu.CompilerParams(vmem_limit_bytes=4 * 1024 * 1024),
        name="store",
    )(*results)
    return (block_out.T, state_next, *[w.transpose(1, 0, 2) for w in windows])


def solution(mesh):
    placed = (
        P(None, ("kv", "tp")),
        P("kv"),
        P("kv", "tp"),
        P("kv", "tp"),
        P("tp", "kv"),
        P("kv"),
        P("kv", "tp"),
        P("kv", "tp"),
        P("kv", "tp"),
        P("kv", "tp"),
        P("kv", "tp"),
        P("tp"),
        P("tp"),
        P("tp"),
        P(None, "tp"),
        P(None, "tp"),
        P(None, "tp"),
        P("kv", None, "tp"),
        P("kv", None, "tp"),
        P("kv", None, "tp"),
        P("kv", "tp", None, None),
        P("tp"),
        P("tp", "kv"),
        P("kv"),
        P("kv", "tp"),
        P("kv", "tp"),
        P("tp", "kv"),
    )
    return jax.shard_map(
        local,
        mesh=mesh,
        in_specs=placed,
        out_specs=(
            P(None, ("kv", "tp")),
            P("kv", "tp", None, None),
            P("kv", None, "tp"),
            P("kv", None, "tp"),
            P("kv", None, "tp"),
        ),
        check_vma=False,
    )
```

```python
import jax
import jax.numpy as jnp
from jax import lax
from jax.experimental import pallas as pl
from jax.experimental.pallas import tpu as pltpu
from jax.sharding import PartitionSpec as P

D = 4096
HEAD_DIM = 64
STATE = 128
EPS = 1e-06

KV = 16
TP = 8
ROWS = 128
FEAT = 256
HID = 1408
INNER = 1024
HEADS = 16
CHUNKS = ((0, 256, "y"), (256, 256, "z"), (512, 256, "y"), (768, 256, "z"), (1024, 256, "y"), (1280, 128, "z"))
GROUP = 512

OTHER = {"y": "z", "z": "y"}
SIZES = {"kv": KV, "tp": TP, "y": 4, "z": 4, "x": 4, "core": 2}

F32 = jnp.float32
BF16 = jnp.bfloat16
MESH = pl.DeviceIdType.MESH


def silu(v):
    return v / (1.0 + jnp.exp(-v))


def dot(a, b):
    return jnp.dot(a, b, preferred_element_type=F32)


class Exchange:
    def __init__(self):
        self.kv = lax.axis_index("kv")
        self.tp = lax.axis_index("tp")
        self.at = {
            "kv": self.kv, "tp": self.tp, "z": self.kv // 4, "y": self.kv % 4, "x": self.tp // 2, "core": self.tp % 2
        }
        self.sent = []

    def peer(self, axis, d):
        z, y = self.at["z"], self.at["y"]
        if axis == "tp":
            place = (self.tp + d) % TP
            return place, (self.kv, place)
        if axis == "kv":
            place = ((z + d // 4) % 4) * 4 + (y + d % 4) % 4
            return place, (place, self.tp)
        place = (self.at[axis] + d) % SIZES[axis]
        if axis == "x":
            return place, (self.kv, place * 2 + self.at["core"])
        if axis == "core":
            return place, (self.kv, self.at["x"] * 2 + place)
        return place, (place * 4 + y if axis == "z" else z * 4 + place, self.tp)

    def each(self, axis, act):
        count = SIZES[axis]
        if count < KV:
            for d in range(1, count):
                act(d)
        else:

            def step(d, c):
                act(d)
                return c

            lax.fori_loop(1, count, step, 0)

    def barrier(self):
        bar = pltpu.get_barrier_semaphore()
        for axis in ("tp", "kv"):
            self.each(
                axis,
                lambda d: pl.semaphore_signal(
                    bar, inc=1, device_id=self.peer(axis, d)[1], device_id_type=MESH
                ),
            )
        with jax.named_scope("barrier"):
            pl.semaphore_wait(bar, KV + TP - 2)

    def copies(self, axis, src_for, dst_for, sems):
        def act(d):
            place, device = self.peer(axis, d)
            pltpu.make_async_remote_copy(
                src_for(place), dst_for(d), sems.at[0], sems.at[1], device_id=device, device_id_type=MESH
            ).start()

        with jax.named_scope("send_" + axis):
            self.each(axis, act)

    def scatter(self, axis, src, dst, sems):
        self.copies(axis, lambda place: src.at[place], lambda d: dst.at[d - 1], sems)
        self.sent.append((dst, sems))

    def spread(self, axis, buf, sems):
        mine = buf.at[self.at[axis]]
        self.copies(axis, lambda place: mine, lambda d: mine, sems)
        self.sent.append((buf.at[pl.ds(0, SIZES[axis] - 1)], sems))

    def arrived(self, dst, sems):
        with jax.named_scope("wait"):
            pltpu.make_async_copy(dst, dst, sems.at[1]).wait()

    def arrived_all(self, buf, sems):
        self.arrived(buf.at[pl.ds(0, buf.shape[0] - 1)], sems)

    def drain(self):
        with jax.named_scope("drain"):
            for dst, sems in self.sent:
                pltpu.make_async_copy(dst, dst, sems.at[0]).wait()


def store_blocks(ref, lo, value, axis):
    size = value.shape[1]
    value = value.reshape(4, 4, 8, size).astype(BF16)
    if axis == "z":
        ref[:, :, :, lo : lo + size] = value
    else:
        for p in range(4):
            ref[p, :, :, lo : lo + size] = value[:, p]


def plus(total, recv):
    for d in range(recv.shape[0]):
        total = total + recv[d].astype(F32)
    return total


def lift(cur, gain_ref):
    wide = cur.astype(F32)
    squares = jnp.sum(wide * wide, axis=1, keepdims=True)
    lifted = (wide * gain_ref[...].reshape(1, FEAT).astype(F32)).astype(BF16)
    return lifted, squares


def half_channel(ex, cur, which, vmem, loaded, bufs, scale_ref, sem, sem_sq):
    gain, gate, up, down = (which + end for end in ("_gain", "_gate", "_up", "_down"))
    squares_buf, *bufs = bufs
    count = len(CHUNKS)
    first, got, second, hid = (bufs[count * k : count * k + count] for k in range(4))
    loaded(gain)
    lifted, squares = lift(cur, vmem[gain])
    loaded(gate, up)
    for i, (lo, size, axis) in enumerate(CHUNKS):
        store_blocks(first[i], 0, dot(lifted, vmem[gate][:, lo : lo + size]), axis)
        store_blocks(first[i], size, dot(lifted, vmem[up][:, lo : lo + size]), axis)
        ex.scatter(axis, first[i], got[i], sem.at[0, i])
    squares_buf[ex.kv] = jnp.transpose(jnp.broadcast_to(squares, (ROWS, 128)))[0:1]
    ex.spread("kv", squares_buf, sem_sq)
    for i, (lo, size, axis) in enumerate(CHUNKS):
        ex.arrived(got[i], sem.at[0, i])
        total = plus(first[i][ex.at[axis]].astype(F32), got[i])
        second[i][ex.at[OTHER[axis]]] = total.astype(BF16)
        ex.spread(OTHER[axis], second[i], sem.at[1, i])
    ex.arrived_all(squares_buf, sem_sq)
    scale = lax.rsqrt(jnp.sum(squares_buf[...], axis=0) / D + EPS)
    scale_ref[...] = jnp.transpose(jnp.broadcast_to(scale, (128, ROWS))).reshape(4, 4, 8, 128)
    scales = {"y": scale_ref[:, ex.at["y"]][:, :, 0:1], "z": scale_ref[ex.at["z"]][:, :, 0:1]}
    for i, (lo, size, axis) in enumerate(CHUNKS):
        ex.arrived_all(second[i], sem.at[1, i])
        total = plus(second[i][0].astype(F32), second[i].at[pl.ds(1, 3)])
        hidden = silu(total[:, :, :size] * scales[axis]) * (total[:, :, size:] * scales[axis])
        hid[i][ex.at[axis]] = hidden.astype(BF16)
        ex.spread(axis, hid[i], sem.at[2, i])
    loaded(down)
    part = None
    for i, (lo, size, axis) in enumerate(CHUNKS):
        ex.arrived_all(hid[i], sem.at[2, i])
        rows = hid[i][...].astype(F32)
        if axis == "y":
            rows = jnp.stack([rows[:, z] for z in range(4)], axis=0)
        p = dot(rows.reshape(ROWS, size).astype(BF16), vmem[down][lo : lo + size, :])
        part = p if part is None else part + p
    return part


def whole_sum(ex, part, cur, factor, bufs, sem):
    send, recv, mine, other = bufs
    send[...] = part.astype(BF16)
    ex.copies("x", lambda place: send, lambda d: recv.at[d - 1], sem.at[0])
    ex.sent.append((recv, sem.at[0]))
    ex.arrived(recv, sem.at[0])
    total = plus(part, recv)
    mine[...] = total
    ex.copies("core", lambda place: mine, lambda d: other, sem.at[1])
    ex.sent.append((other, sem.at[1]))
    ex.arrived(other, sem.at[1])
    return (cur.astype(F32) + factor * (total + other[...])).astype(BF16)


NAMES = (
    "block_in", "before_gain", "before_gate", "before_up", "before_down", "mix_gain", "input_gate",
    "input_value", "input_write", "input_read", "input_step", "step_bias", "decay_log", "skip_gain",
    "value_taps", "write_taps", "read_taps", "value_window", "write_window", "read_window", "scan_state",
    "group_gain", "mixer_out", "after_gain", "after_gate", "after_up", "after_down",
)


def kernel(
    *refs,
):
    count = len(NAMES)
    hbm = dict(zip(NAMES, refs[:count]))
    block_out, state_out, value_next, write_next, read_next = refs[count : count + 5]
    vmem = dict(zip(NAMES, refs[count + 5 : 2 * count + 5]))
    load_sem, *rest = refs[2 * count + 5 :]

    def take(count):
        taken = rest[:count]
        del rest[:count]
        return taken

    packed, scale_ref, olds = take(3)
    a_bufs, b_bufs = take(1 + 4 * len(CHUNKS)), take(1 + 4 * len(CHUNKS))
    tile_send, tile_recv = take(2)
    m_bufs, m_hid = [[take(4) for axis in range(2)] for g in range(2)], take(2)
    t1_bufs, t2_bufs = take(4), take(4)
    t3_own, t3_send, t3_recv = take(3)
    sem_in, sem_a, sem_b, sem_a_sq, sem_b_sq, sem_m, sem_tile, sem_hid, sem_t1, sem_t2, sem_t3 = take(11)
    ex = Exchange()
    loads = {n: pltpu.make_async_copy(hbm[n], vmem[n], load_sem.at[i]) for i, n in enumerate(NAMES) if n != "block_in"}
    mine = pltpu.make_async_copy(hbm["block_in"], packed.at[ex.tp], load_sem.at[0])
    mine.start()
    for copy in loads.values():
        copy.start()

    def loaded(*names):
        with jax.named_scope("loaded"):
            for n in names:
                loads[n].wait()

    ex.barrier()
    mine.wait()
    ex.spread("tp", packed, sem_in)
    ex.arrived_all(packed, sem_in)
    cur = jnp.transpose(packed[...].astype(F32).reshape(FEAT, ROWS)).astype(BF16)

    part = half_channel(ex, cur, "before", vmem, loaded, a_bufs, scale_ref, sem_a, sem_a_sq)
    cur = whole_sum(ex, part, cur, 0.5, t1_bufs, sem_t1)

    loaded("mix_gain", "input_gate", "input_value", "input_write", "input_read", "input_step")
    lifted, squares = lift(cur, vmem["mix_gain"])
    lanes = [slice(GROUP * g, GROUP * g + GROUP) for g in range(2)]
    states = [slice(STATE * g, STATE * g + STATE) for g in range(2)]
    for g in range(2):
        for k, (axis, wide, narrow) in enumerate((("y", "gate", "write"), ("z", "value", "read"))):
            first, got = m_bufs[g][k][:2]
            store_blocks(first, 0, dot(lifted, vmem["input_" + wide][:, lanes[g]]), axis)
            store_blocks(first, GROUP, dot(lifted, vmem["input_" + narrow][:, states[g]]), axis)
            ex.scatter(axis, first, got, sem_m.at[g, k, 0])
        if g == 0:
            place = lax.broadcasted_iota(jnp.int32, (128, HEADS), 0)
            head = lax.broadcasted_iota(jnp.int32, (128, HEADS), 1)
            spots = jnp.where(place == head, 1.0, 0.0).astype(BF16)
            step_w = dot(spots, vmem["input_step"][...]).astype(BF16)
            step = lax.dot_general(lifted, step_w, (((1,), (1,)), ((), ())), preferred_element_type=F32)
            lane = lax.broadcasted_iota(jnp.int32, (ROWS, 128), 1)
            tile_send[...] = jnp.where(lane < HEADS, step, squares).reshape(KV, 8, 128)
            ex.scatter("kv", tile_send, tile_recv, sem_tile)
    loaded("step_bias", "decay_log", "skip_gain", "group_gain", "scan_state")
    with jax.named_scope("olds"):
        for g in range(2):
            for r in range(8):
                old = vmem["scan_state"][r, 8 * g : 8 * g + 8].reshape(GROUP, STATE)
                olds[g, :, STATE * r : STATE * r + STATE] = old.astype(BF16)
    loaded(*(a + b for a in ("value", "write", "read") for b in ("_taps", "_window")))
    for g in range(2):
        for k, axis in enumerate(("y", "z")):
            first, got, second, last = m_bufs[g][k]
            ex.arrived(got, sem_m.at[g, k, 0])
            second[...] = plus(first[ex.at[axis]].astype(F32), got).astype(BF16)
            ex.scatter(OTHER[axis], second, last, sem_m.at[g, k, 1])

    ex.arrived(tile_recv, sem_tile)
    tile = plus(tile_send[ex.kv], tile_recv)
    scale = lax.rsqrt(tile[:, HEADS : HEADS + 1] / D + EPS)
    raw = tile[:, :HEADS] * scale + vmem["step_bias"][...].reshape(1, HEADS)
    step_size = jnp.maximum(raw, 0.0) + jnp.log1p(jnp.exp(-jnp.abs(raw)))
    decay = jnp.exp(-step_size * jnp.exp(vmem["decay_log"][...].reshape(1, HEADS)))
    skip = jnp.broadcast_to(vmem["skip_gain"][...].reshape(1, HEADS), (8, HEADS))
    of = lax.broadcasted_iota(jnp.int32, (HEADS, INNER), 1) // HEAD_DIM
    row = lax.broadcasted_iota(jnp.int32, (HEADS, INNER), 0)
    heads = jnp.dot(
        jnp.concatenate([step_size, decay, skip], axis=0),
        jnp.where(of == row, 1.0, 0.0),
        preferred_element_type=F32,
        precision=lax.Precision.HIGHEST,
    )
    gain = vmem["group_gain"][...].reshape(1, INNER).astype(F32)
    updates = []
    for g in range(2):
        sums = []
        for k, axis in enumerate(("y", "z")):
            first, got, second, last = m_bufs[g][k]
            ex.arrived(last, sem_m.at[g, k, 1])
            sums.append(plus(second[ex.at[OTHER[axis]]].astype(F32), last) * scale)
        next_refs = {"value": value_next, "write": write_next, "read": read_next}

        def conv(fresh, kind, at):
            window = [vmem[kind + "_window"][i, :, at] for i in range(3)] + [fresh.astype(BF16)]
            taps = vmem[kind + "_taps"][:, at].astype(F32)
            acc = None
            for i in range(4):
                if i:
                    next_refs[kind][i - 1, :, at] = window[i]
                term = window[i].astype(F32) * taps[i : i + 1]
                acc = term if acc is None else acc + term
            return silu(acc)

        gate_rows = sums[0][:, :GROUP].astype(BF16).astype(F32)
        write = conv(sums[0][:, GROUP:], "write", states[g])
        value = conv(sums[1][:, :GROUP], "value", lanes[g])
        read = conv(sums[1][:, GROUP:], "read", states[g])
        step_x = heads[0:8, lanes[g]] * value
        row = lax.broadcasted_iota(jnp.int32, (8, STATE), 0)
        reads = jnp.concatenate([jnp.where(row == r, read, 0.0) for r in range(8)], axis=1).astype(BF16)
        kept = lax.dot_general(reads, olds[g], (((1,), (1,)), ((), ())), preferred_element_type=F32)
        meet = jnp.sum(write * read, axis=1, keepdims=True)
        readout = heads[8:16, lanes[g]] * kept + step_x * meet + heads[16:24, lanes[g]] * value
        gated = readout * silu(gate_rows)
        mean = jnp.sum(gated * gated, axis=1, keepdims=True) / GROUP
        m_hid[g][ex.kv] = (gated * lax.rsqrt(mean + EPS) * gain[:, lanes[g]]).astype(BF16)
        ex.spread("kv", m_hid[g], sem_hid.at[g])
        updates.append((step_x, heads[8:16, lanes[g]], write))
    with jax.named_scope("update"):
        for g, (step_x, kept, write) in enumerate(updates):
            across = jnp.transpose(jnp.concatenate([step_x, kept], axis=0))
            for r in range(8):
                old = vmem["scan_state"][r, 8 * g : 8 * g + 8].reshape(GROUP, STATE)
                new = across[:, 8 + r : 9 + r] * old + across[:, r : r + 1] * write[r : r + 1]
                state_out[r, 8 * g : 8 * g + 8] = new.reshape(8, HEAD_DIM, STATE)
    loaded("mixer_out")
    part = None
    for g in range(2):
        ex.arrived_all(m_hid[g], sem_hid.at[g])
        rows = m_hid[g][...].astype(F32).reshape(ROWS, GROUP).astype(BF16)
        p = dot(rows, vmem["mixer_out"][lanes[g], :])
        part = p if part is None else part + p
    cur = whole_sum(ex, part, cur, 1.0, t2_bufs, sem_t2)

    part = half_channel(ex, cur, "after", vmem, loaded, b_bufs, scale_ref, sem_b, sem_b_sq)
    columns = jnp.transpose(part).reshape(TP, 32, ROWS)
    t3_own[...] = columns
    t3_send[...] = columns.astype(BF16)
    ex.scatter("tp", t3_send, t3_recv, sem_t3)
    total = t3_own[ex.tp]
    t3_own[...] = jnp.transpose(cur.astype(F32)).reshape(TP, 32, ROWS)
    ex.arrived(t3_recv, sem_t3)
    total = plus(total, t3_recv)
    block_out[...] = (t3_own[ex.tp] + 0.5 * total).astype(BF16)
    ex.drain()


def store(*refs):
    srcs, dsts, sem = refs[: (len(refs) - 1) // 2], refs[(len(refs) - 1) // 2 : -1], refs[-1]
    copies = [pltpu.make_async_copy(s, d, sem.at[i]) for i, (s, d) in enumerate(zip(srcs, dsts))]
    for copy in copies:
        copy.start()
    for copy in copies:
        copy.wait()


def local(*args):
    named = dict(zip(NAMES, args))
    named["block_in"] = named["block_in"].T
    named["input_step"] = named["input_step"].T
    for kind in ("value", "write", "read"):
        named[kind + "_window"] = named[kind + "_window"].transpose(1, 0, 2)
    operands = [pltpu.with_memory_space_constraint(named[n], pltpu.HBM) for n in NAMES]
    vmem = pl.BlockSpec(memory_space=pltpu.VMEM)
    hbm = pl.BlockSpec(memory_space=pltpu.HBM)

    def v(*shape, dtype=BF16):
        return pltpu.VMEM(shape, dtype)

    def parts(lead, scale, chunks):
        return [v(*lead, 8, scale * size) for _, size, _ in chunks]

    channel = [
        v(KV, 1, ROWS, dtype=F32),
        *parts((4, 4), 2, CHUNKS), *parts((3, 4), 2, CHUNKS), *parts((4, 4), 2, CHUNKS), *parts((4, 4), 1, CHUNKS),
    ]
    tp_sum = [v(ROWS, FEAT), v(3, ROWS, FEAT), v(ROWS, FEAT, dtype=F32), v(ROWS, FEAT, dtype=F32)]
    width = GROUP + STATE
    mixer = 4 * [v(4, 4, 8, width), v(3, 4, 8, width), v(4, 8, width), v(3, 8, width)] + 2 * [v(KV, 8, GROUP)]
    sems = pltpu.SemaphoreType.DMA
    shapes = (
        jax.ShapeDtypeStruct((32, ROWS), BF16),
        jax.ShapeDtypeStruct(named["scan_state"].shape, F32),
        jax.ShapeDtypeStruct((3, 8, INNER), BF16),
        jax.ShapeDtypeStruct((3, 8, 256), BF16),
        jax.ShapeDtypeStruct((3, 8, 256), BF16),
    )
    results = pl.pallas_call(
        kernel,
        out_shape=shapes,
        in_specs=[hbm] * len(operands),
        out_specs=(vmem,) * 5,
        scratch_shapes=[
            *[v(*a.shape, dtype=a.dtype) for a in operands],
            sems((len(NAMES),)),
            v(TP, 32, 128), v(4, 4, 8, 128, dtype=F32), v(2, GROUP, 8 * STATE),
            *channel, *channel,
            v(KV, 8, 128, dtype=F32), v(KV - 1, 8, 128, dtype=F32), *mixer,
            *tp_sum, *tp_sum,
            v(TP, 32, 128, dtype=F32), v(TP, 32, 128), v(TP - 1, 32, 128),
            sems((2,)), sems((3, len(CHUNKS), 2)), sems((3, len(CHUNKS), 2)), sems((2,)), sems((2,)),
            sems((2, 2, 2, 2)), sems((2,)), sems((2, 2)), sems((2, 2)), sems((2, 2)), sems((2,)),
        ],
        compiler_params=pltpu.CompilerParams(
            collective_id=0, has_side_effects=True, vmem_limit_bytes=40 * 1024 * 1024
        ),
        name="layer",
    )(*operands)
    block_out, state_next, *windows = pl.pallas_call(
        store,
        out_shape=shapes,
        in_specs=[vmem] * 5,
        out_specs=(hbm,) * 5,
        scratch_shapes=[sems((5,))],
        compiler_params=pltpu.CompilerParams(vmem_limit_bytes=4 * 1024 * 1024),
        name="store",
    )(*results)
    return (block_out.T, state_next, *[w.transpose(1, 0, 2) for w in windows])


def solution(mesh):
    placed = (
        P(None, ("kv", "tp")),
        P("kv"),
        P("kv", "tp"),
        P("kv", "tp"),
        P("tp", "kv"),
        P("kv"),
        P("kv", "tp"),
        P("kv", "tp"),
        P("kv", "tp"),
        P("kv", "tp"),
        P("kv", "tp"),
        P("tp"),
        P("tp"),
        P("tp"),
        P(None, "tp"),
        P(None, "tp"),
        P(None, "tp"),
        P("kv", None, "tp"),
        P("kv", None, "tp"),
        P("kv", None, "tp"),
        P("kv", "tp", None, None),
        P("tp"),
        P("tp", "kv"),
        P("kv"),
        P("kv", "tp"),
        P("kv", "tp"),
        P("tp", "kv"),
    )
    return jax.shard_map(
        local,
        mesh=mesh,
        in_specs=placed,
        out_specs=(
            P(None, ("kv", "tp")),
            P("kv", "tp", None, None),
            P("kv", None, "tp"),
            P("kv", None, "tp"),
            P("kv", None, "tp"),
        ),
        check_vma=False,
    )
```

```python
import jax
import jax.numpy as jnp
from jax import lax
from jax.experimental import pallas as pl
from jax.experimental.pallas import tpu as pltpu
from jax.sharding import PartitionSpec as P

D = 4096
HEAD_DIM = 64
STATE = 128
EPS = 1e-06

KV = 16
TP = 8
ROWS = 128
FEAT = 256
HID = 1408
INNER = 1024
HEADS = 16
CHUNKS = ((0, 128, "y"), (128, 128, "z"), (256, 128, "y"), (384, 128, "z"), (512, 128, "y"), (640, 128, "z"), (768, 128, "y"), (896, 128, "z"), (1024, 128, "y"), (1152, 128, "z"), (1280, 128, "y"))
GROUP = 512

OTHER = {"y": "z", "z": "y"}
SIZES = {"kv": KV, "tp": TP, "y": 4, "z": 4, "x": 4, "core": 2}

F32 = jnp.float32
BF16 = jnp.bfloat16
MESH = pl.DeviceIdType.MESH


def silu(v):
    return v / (1.0 + jnp.exp(-v))


def dot(a, b):
    return jnp.dot(a, b, preferred_element_type=F32)


HOPS = (0, 1, 2, 1)
FARTHEST_FIRST = tuple(sorted(range(1, KV), key=lambda d: -HOPS[d // 4] - HOPS[d % 4]))


class Exchange:
    def __init__(self):
        self.kv = lax.axis_index("kv")
        self.tp = lax.axis_index("tp")
        self.at = {
            "kv": self.kv, "tp": self.tp, "z": self.kv // 4, "y": self.kv % 4, "x": self.tp // 2, "core": self.tp % 2
        }
        self.sent = []

    def peer(self, axis, d):
        z, y = self.at["z"], self.at["y"]
        if axis == "tp":
            place = (self.tp + d) % TP
            return place, (self.kv, place)
        if axis == "kv":
            place = ((z + d // 4) % 4) * 4 + (y + d % 4) % 4
            return place, (place, self.tp)
        place = (self.at[axis] + d) % SIZES[axis]
        if axis == "x":
            return place, (self.kv, place * 2 + self.at["core"])
        if axis == "core":
            return place, (self.kv, self.at["x"] * 2 + place)
        return place, (place * 4 + y if axis == "z" else z * 4 + place, self.tp)

    def each(self, axis, act):
        for d in FARTHEST_FIRST if axis == "kv" else range(1, SIZES[axis]):
            act(d)

    def barrier(self):
        bar = pltpu.get_barrier_semaphore()
        for axis in ("tp", "y", "z"):
            self.each(
                axis,
                lambda d: pl.semaphore_signal(
                    bar, inc=1, device_id=self.peer(axis, d)[1], device_id_type=MESH
                ),
            )
        with jax.named_scope("barrier"):
            pl.semaphore_wait(bar, TP - 1 + 3 + 3)

    def copies(self, axis, src_for, dst_for, sems):
        def act(d):
            place, device = self.peer(axis, d)
            pltpu.make_async_remote_copy(
                src_for(place), dst_for(d), sems.at[0], sems.at[1], device_id=device, device_id_type=MESH
            ).start()

        with jax.named_scope("send_" + axis):
            self.each(axis, act)

    def scatter(self, axis, src, dst, sems):
        self.copies(axis, lambda place: src.at[place], lambda d: dst.at[d - 1], sems)
        self.sent.append((dst, sems))

    def spread(self, axis, buf, sems):
        mine = buf.at[self.at[axis]]
        self.copies(axis, lambda place: mine, lambda d: mine, sems)
        self.sent.append((buf.at[pl.ds(0, SIZES[axis] - 1)], sems))

    def arrived(self, dst, sems):
        with jax.named_scope("wait"):
            pltpu.make_async_copy(dst, dst, sems.at[1]).wait()

    def arrived_all(self, buf, sems):
        self.arrived(buf.at[pl.ds(0, buf.shape[0] - 1)], sems)

    def drain(self):
        with jax.named_scope("drain"):
            for dst, sems in self.sent:
                pltpu.make_async_copy(dst, dst, sems.at[0]).wait()


def store_blocks(ref, lo, value, axis):
    size = value.shape[1]
    value = value.reshape(4, 4, 8, size).astype(BF16)
    if axis == "z":
        ref[:, :, :, lo : lo + size] = value
    else:
        for p in range(4):
            ref[p, :, :, lo : lo + size] = value[:, p]


def plus(total, recv):
    for d in range(recv.shape[0]):
        total = total + recv[d].astype(F32)
    return total


def lift(cur, gain_ref):
    wide = cur.astype(F32)
    squares = jnp.sum(wide * wide, axis=1, keepdims=True)
    lifted = (wide * gain_ref[...].reshape(1, FEAT).astype(F32)).astype(BF16)
    return lifted, squares


def half_channel(ex, cur, which, vmem, loaded, bufs, scale_ref, sem, sem_sq):
    gain, gate, up, down = (which + end for end in ("_gain", "_gate", "_up", "_down"))
    squares_bufs, bufs = bufs[:2], bufs[2:]
    count = len(CHUNKS)
    first, got, second, hid = (bufs[count * k : count * k + count] for k in range(4))
    loaded(gain)
    lifted, squares = lift(cur, vmem[gain])
    squares_bufs[0][ex.at["y"]] = jnp.transpose(jnp.broadcast_to(squares, (ROWS, 128)))[0:1]
    ex.spread("y", squares_bufs[0], sem_sq.at[0])
    loaded(gate, up)
    for i, (lo, size, axis) in enumerate(CHUNKS):
        store_blocks(first[i], 0, dot(lifted, vmem[gate][:, lo : lo + size]), axis)
        store_blocks(first[i], size, dot(lifted, vmem[up][:, lo : lo + size]), axis)
        ex.scatter(axis, first[i], got[i], sem.at[0, i])
    ex.arrived_all(squares_bufs[0], sem_sq.at[0])
    squares_bufs[1][ex.at["z"]] = jnp.sum(squares_bufs[0][...], axis=0)
    ex.spread("z", squares_bufs[1], sem_sq.at[1])
    for i, (lo, size, axis) in enumerate(CHUNKS):
        ex.arrived(got[i], sem.at[0, i])
        total = plus(first[i][ex.at[axis]].astype(F32), got[i])
        second[i][ex.at[OTHER[axis]]] = total.astype(BF16)
        ex.spread(OTHER[axis], second[i], sem.at[1, i])
    ex.arrived_all(squares_bufs[1], sem_sq.at[1])
    scale = lax.rsqrt(jnp.sum(squares_bufs[1][...], axis=0) / D + EPS)
    scale_ref[...] = jnp.transpose(jnp.broadcast_to(scale, (128, ROWS))).reshape(4, 4, 8, 128)
    scales = {"y": scale_ref[:, ex.at["y"]][:, :, 0:1], "z": scale_ref[ex.at["z"]][:, :, 0:1]}
    for i, (lo, size, axis) in enumerate(CHUNKS):
        ex.arrived_all(second[i], sem.at[1, i])
        total = plus(second[i][0].astype(F32), second[i].at[pl.ds(1, 3)])
        hidden = silu(total[:, :, :size] * scales[axis]) * (total[:, :, size:] * scales[axis])
        hid[i][ex.at[axis]] = hidden.astype(BF16)
        ex.spread(axis, hid[i], sem.at[2, i])
    loaded(down)
    part = None
    for i, (lo, size, axis) in enumerate(CHUNKS):
        ex.arrived_all(hid[i], sem.at[2, i])
        rows = hid[i][...].astype(F32)
        if axis == "y":
            rows = jnp.stack([rows[:, z] for z in range(4)], axis=0)
        p = dot(rows.reshape(ROWS, size).astype(BF16), vmem[down][lo : lo + size, :])
        part = p if part is None else part + p
    return part


def whole_sum(ex, part, cur, factor, bufs, sem):
    send, recv, mine, other = bufs
    send[...] = part.astype(BF16)
    ex.copies("x", lambda place: send, lambda d: recv.at[d - 1], sem.at[0])
    ex.sent.append((recv, sem.at[0]))
    ex.arrived(recv, sem.at[0])
    total = plus(part, recv)
    mine[...] = total
    ex.copies("core", lambda place: mine, lambda d: other, sem.at[1])
    ex.sent.append((other, sem.at[1]))
    ex.arrived(other, sem.at[1])
    return (cur.astype(F32) + factor * (total + other[...])).astype(BF16)


NAMES = (
    "block_in", "before_gain", "before_gate", "before_up", "before_down", "mix_gain", "input_gate",
    "input_value", "input_write", "input_read", "input_step", "step_bias", "decay_log", "skip_gain",
    "value_taps", "write_taps", "read_taps", "value_window", "write_window", "read_window", "scan_state",
    "group_gain", "mixer_out", "after_gain", "after_gate", "after_up", "after_down",
)


def kernel(
    *refs,
):
    count = len(NAMES)
    hbm = dict(zip(NAMES, refs[:count]))
    block_out, state_out, value_next, write_next, read_next = refs[count : count + 5]
    vmem = dict(zip(NAMES, refs[count + 5 : 2 * count + 5]))
    load_sem, *rest = refs[2 * count + 5 :]

    def take(count):
        taken = rest[:count]
        del rest[:count]
        return taken

    packed, scale_ref, olds = take(3)
    a_bufs, b_bufs = take(2 + 4 * len(CHUNKS)), take(2 + 4 * len(CHUNKS))
    tile_send, tile_recv = take(2)
    m_bufs, m_hid = [[take(4) for axis in range(2)] for g in range(2)], take(2)
    t1_bufs, t2_bufs = take(4), take(4)
    t3_own, t3_send, t3_recv = take(3)
    sem_in, sem_a, sem_b, sem_a_sq, sem_b_sq, sem_m, sem_tile, sem_hid, sem_t1, sem_t2, sem_t3 = take(11)
    ex = Exchange()
    loads = {n: pltpu.make_async_copy(hbm[n], vmem[n], load_sem.at[i]) for i, n in enumerate(NAMES) if n != "block_in"}
    mine = pltpu.make_async_copy(hbm["block_in"], packed.at[ex.tp], load_sem.at[0])
    mine.start()
    for copy in loads.values():
        copy.start()

    def loaded(*names):
        with jax.named_scope("loaded"):
            for n in names:
                loads[n].wait()

    ex.barrier()
    mine.wait()
    ex.spread("tp", packed, sem_in)
    ex.arrived_all(packed, sem_in)
    cur = jnp.transpose(packed[...].astype(F32).reshape(FEAT, ROWS)).astype(BF16)

    part = half_channel(ex, cur, "before", vmem, loaded, a_bufs, scale_ref, sem_a, sem_a_sq)
    cur = whole_sum(ex, part, cur, 0.5, t1_bufs, sem_t1)

    loaded("mix_gain", "input_gate", "input_value", "input_write", "input_read", "input_step")
    lifted, squares = lift(cur, vmem["mix_gain"])
    lanes = [slice(GROUP * g, GROUP * g + GROUP) for g in range(2)]
    states = [slice(STATE * g, STATE * g + STATE) for g in range(2)]
    for g in range(2):
        for k, (axis, wide, narrow) in enumerate((("y", "gate", "write"), ("z", "value", "read"))):
            first, got = m_bufs[g][k][:2]
            store_blocks(first, 0, dot(lifted, vmem["input_" + wide][:, lanes[g]]), axis)
            store_blocks(first, GROUP, dot(lifted, vmem["input_" + narrow][:, states[g]]), axis)
            ex.scatter(axis, first, got, sem_m.at[g, k, 0])
        if g == 0:
            place = lax.broadcasted_iota(jnp.int32, (128, HEADS), 0)
            head = lax.broadcasted_iota(jnp.int32, (128, HEADS), 1)
            spots = jnp.where(place == head, 1.0, 0.0).astype(BF16)
            step_w = dot(spots, vmem["input_step"][...]).astype(BF16)
            step = lax.dot_general(lifted, step_w, (((1,), (1,)), ((), ())), preferred_element_type=F32)
            lane = lax.broadcasted_iota(jnp.int32, (ROWS, 128), 1)
            tile_send[...] = jnp.where(lane < HEADS, step, squares).reshape(KV, 8, 128)
            ex.scatter("kv", tile_send, tile_recv, sem_tile)
    loaded("step_bias", "decay_log", "skip_gain", "group_gain", "scan_state")
    with jax.named_scope("olds"):
        for g in range(2):
            for r in range(8):
                old = vmem["scan_state"][r, 8 * g : 8 * g + 8].reshape(GROUP, STATE)
                olds[g, :, STATE * r : STATE * r + STATE] = old.astype(BF16)
    loaded(*(a + b for a in ("value", "write", "read") for b in ("_taps", "_window")))
    for g in range(2):
        for k, axis in enumerate(("y", "z")):
            first, got, second, last = m_bufs[g][k]
            ex.arrived(got, sem_m.at[g, k, 0])
            second[...] = plus(first[ex.at[axis]].astype(F32), got).astype(BF16)
            ex.scatter(OTHER[axis], second, last, sem_m.at[g, k, 1])

    ex.arrived(tile_recv, sem_tile)
    tile = plus(tile_send[ex.kv], tile_recv)
    scale = lax.rsqrt(tile[:, HEADS : HEADS + 1] / D + EPS)
    raw = tile[:, :HEADS] * scale + vmem["step_bias"][...].reshape(1, HEADS)
    step_size = jnp.maximum(raw, 0.0) + jnp.log1p(jnp.exp(-jnp.abs(raw)))
    decay = jnp.exp(-step_size * jnp.exp(vmem["decay_log"][...].reshape(1, HEADS)))
    skip = jnp.broadcast_to(vmem["skip_gain"][...].reshape(1, HEADS), (8, HEADS))
    of = lax.broadcasted_iota(jnp.int32, (HEADS, INNER), 1) // HEAD_DIM
    row = lax.broadcasted_iota(jnp.int32, (HEADS, INNER), 0)
    heads = jnp.dot(
        jnp.concatenate([step_size, decay, skip], axis=0),
        jnp.where(of == row, 1.0, 0.0),
        preferred_element_type=F32,
        precision=lax.Precision.HIGHEST,
    )
    gain = vmem["group_gain"][...].reshape(1, INNER).astype(F32)
    updates = []
    for g in range(2):
        sums = []
        for k, axis in enumerate(("y", "z")):
            first, got, second, last = m_bufs[g][k]
            ex.arrived(last, sem_m.at[g, k, 1])
            sums.append(plus(second[ex.at[OTHER[axis]]].astype(F32), last) * scale)
        next_refs = {"value": value_next, "write": write_next, "read": read_next}

        def conv(fresh, kind, at):
            window = [vmem[kind + "_window"][i, :, at] for i in range(3)] + [fresh.astype(BF16)]
            taps = vmem[kind + "_taps"][:, at].astype(F32)
            acc = None
            for i in range(4):
                if i:
                    next_refs[kind][i - 1, :, at] = window[i]
                term = window[i].astype(F32) * taps[i : i + 1]
                acc = term if acc is None else acc + term
            return silu(acc)

        gate_rows = sums[0][:, :GROUP].astype(BF16).astype(F32)
        write = conv(sums[0][:, GROUP:], "write", states[g])
        value = conv(sums[1][:, :GROUP], "value", lanes[g])
        read = conv(sums[1][:, GROUP:], "read", states[g])
        step_x = heads[0:8, lanes[g]] * value
        row = lax.broadcasted_iota(jnp.int32, (8, STATE), 0)
        reads = jnp.concatenate([jnp.where(row == r, read, 0.0) for r in range(8)], axis=1).astype(BF16)
        kept = lax.dot_general(reads, olds[g], (((1,), (1,)), ((), ())), preferred_element_type=F32)
        meet = jnp.sum(write * read, axis=1, keepdims=True)
        readout = heads[8:16, lanes[g]] * kept + step_x * meet + heads[16:24, lanes[g]] * value
        gated = readout * silu(gate_rows)
        mean = jnp.sum(gated * gated, axis=1, keepdims=True) / GROUP
        m_hid[g][ex.kv] = (gated * lax.rsqrt(mean + EPS) * gain[:, lanes[g]]).astype(BF16)
        ex.spread("kv", m_hid[g], sem_hid.at[g])
        updates.append((step_x, heads[8:16, lanes[g]], write))
    with jax.named_scope("update"):
        for g, (step_x, kept, write) in enumerate(updates):
            across = jnp.transpose(jnp.concatenate([step_x, kept], axis=0))
            for r in range(8):
                old = vmem["scan_state"][r, 8 * g : 8 * g + 8].reshape(GROUP, STATE)
                new = across[:, 8 + r : 9 + r] * old + across[:, r : r + 1] * write[r : r + 1]
                state_out[r, 8 * g : 8 * g + 8] = new.reshape(8, HEAD_DIM, STATE)
    loaded("mixer_out")
    part = None
    for g in range(2):
        ex.arrived_all(m_hid[g], sem_hid.at[g])
        rows = m_hid[g][...].astype(F32).reshape(ROWS, GROUP).astype(BF16)
        p = dot(rows, vmem["mixer_out"][lanes[g], :])
        part = p if part is None else part + p
    cur = whole_sum(ex, part, cur, 1.0, t2_bufs, sem_t2)

    part = half_channel(ex, cur, "after", vmem, loaded, b_bufs, scale_ref, sem_b, sem_b_sq)
    columns = jnp.transpose(part).reshape(TP, 32, ROWS)
    t3_own[...] = columns
    t3_send[...] = columns.astype(BF16)
    ex.scatter("tp", t3_send, t3_recv, sem_t3)
    total = t3_own[ex.tp]
    t3_own[...] = jnp.transpose(cur.astype(F32)).reshape(TP, 32, ROWS)
    ex.arrived(t3_recv, sem_t3)
    total = plus(total, t3_recv)
    block_out[...] = (t3_own[ex.tp] + 0.5 * total).astype(BF16)
    ex.drain()


def store(*refs):
    srcs, dsts, sem = refs[: (len(refs) - 1) // 2], refs[(len(refs) - 1) // 2 : -1], refs[-1]
    copies = [pltpu.make_async_copy(s, d, sem.at[i]) for i, (s, d) in enumerate(zip(srcs, dsts))]
    for copy in copies:
        copy.start()
    for copy in copies:
        copy.wait()


def local(*args):
    named = dict(zip(NAMES, args))
    named["block_in"] = named["block_in"].T
    named["input_step"] = named["input_step"].T
    for kind in ("value", "write", "read"):
        named[kind + "_window"] = named[kind + "_window"].transpose(1, 0, 2)
    operands = [pltpu.with_memory_space_constraint(named[n], pltpu.HBM) for n in NAMES]
    vmem = pl.BlockSpec(memory_space=pltpu.VMEM)
    hbm = pl.BlockSpec(memory_space=pltpu.HBM)

    def v(*shape, dtype=BF16):
        return pltpu.VMEM(shape, dtype)

    def parts(lead, scale, chunks):
        return [v(*lead, 8, scale * size) for _, size, _ in chunks]

    channel = [
        v(4, 1, ROWS, dtype=F32), v(4, 1, ROWS, dtype=F32),
        *parts((4, 4), 2, CHUNKS), *parts((3, 4), 2, CHUNKS), *parts((4, 4), 2, CHUNKS), *parts((4, 4), 1, CHUNKS),
    ]
    tp_sum = [v(ROWS, FEAT), v(3, ROWS, FEAT), v(ROWS, FEAT, dtype=F32), v(ROWS, FEAT, dtype=F32)]
    width = GROUP + STATE
    mixer = 4 * [v(4, 4, 8, width), v(3, 4, 8, width), v(4, 8, width), v(3, 8, width)] + 2 * [v(KV, 8, GROUP)]
    sems = pltpu.SemaphoreType.DMA
    shapes = (
        jax.ShapeDtypeStruct((32, ROWS), BF16),
        jax.ShapeDtypeStruct(named["scan_state"].shape, F32),
        jax.ShapeDtypeStruct((3, 8, INNER), BF16),
        jax.ShapeDtypeStruct((3, 8, 256), BF16),
        jax.ShapeDtypeStruct((3, 8, 256), BF16),
    )
    results = pl.pallas_call(
        kernel,
        out_shape=shapes,
        in_specs=[hbm] * len(operands),
        out_specs=(vmem,) * 5,
        scratch_shapes=[
            *[v(*a.shape, dtype=a.dtype) for a in operands],
            sems((len(NAMES),)),
            v(TP, 32, 128), v(4, 4, 8, 128, dtype=F32), v(2, GROUP, 8 * STATE),
            *channel, *channel,
            v(KV, 8, 128, dtype=F32), v(KV - 1, 8, 128, dtype=F32), *mixer,
            *tp_sum, *tp_sum,
            v(TP, 32, 128, dtype=F32), v(TP, 32, 128), v(TP - 1, 32, 128),
            sems((2,)), sems((3, len(CHUNKS), 2)), sems((3, len(CHUNKS), 2)), sems((2, 2)), sems((2, 2)),
            sems((2, 2, 2, 2)), sems((2,)), sems((2, 2)), sems((2, 2)), sems((2, 2)), sems((2,)),
        ],
        compiler_params=pltpu.CompilerParams(
            collective_id=0, has_side_effects=True, vmem_limit_bytes=40 * 1024 * 1024
        ),
        name="layer",
    )(*operands)
    block_out, state_next, *windows = pl.pallas_call(
        store,
        out_shape=shapes,
        in_specs=[vmem] * 5,
        out_specs=(hbm,) * 5,
        scratch_shapes=[sems((5,))],
        compiler_params=pltpu.CompilerParams(vmem_limit_bytes=4 * 1024 * 1024),
        name="store",
    )(*results)
    return (block_out.T, state_next, *[w.transpose(1, 0, 2) for w in windows])


def solution(mesh):
    placed = (
        P(None, ("kv", "tp")),
        P("kv"),
        P("kv", "tp"),
        P("kv", "tp"),
        P("tp", "kv"),
        P("kv"),
        P("kv", "tp"),
        P("kv", "tp"),
        P("kv", "tp"),
        P("kv", "tp"),
        P("kv", "tp"),
        P("tp"),
        P("tp"),
        P("tp"),
        P(None, "tp"),
        P(None, "tp"),
        P(None, "tp"),
        P("kv", None, "tp"),
        P("kv", None, "tp"),
        P("kv", None, "tp"),
        P("kv", "tp", None, None),
        P("tp"),
        P("tp", "kv"),
        P("kv"),
        P("kv", "tp"),
        P("kv", "tp"),
        P("tp", "kv"),
    )
    return jax.shard_map(
        local,
        mesh=mesh,
        in_specs=placed,
        out_specs=(
            P(None, ("kv", "tp")),
            P("kv", "tp", None, None),
            P("kv", None, "tp"),
            P("kv", None, "tp"),
            P("kv", None, "tp"),
        ),
        check_vma=False,
    )
```

```python
import jax
import jax.numpy as jnp
from jax import lax
from jax.experimental import pallas as pl
from jax.experimental.pallas import tpu as pltpu
from jax.sharding import PartitionSpec as P

D = 4096
HEAD_DIM = 64
STATE = 128
EPS = 1e-06

KV = 16
TP = 8
ROWS = 128
FEAT = 256
HID = 1408
INNER = 1024
HEADS = 16
CHUNKS = ((0, 128, "y"), (128, 128, "z"), (256, 128, "y"), (384, 128, "z"), (512, 128, "y"), (640, 128, "z"), (768, 128, "y"), (896, 128, "z"), (1024, 128, "y"), (1152, 128, "z"), (1280, 128, "y"))
GROUP = 512
MIXED = (
    ("y", (("gate", 0, 512), ("write", 0, 128))),
    ("z", (("value", 0, 512), ("read", 0, 128))),
)
WIDTHS = {"gate": 512, "value": 512, "write": 128, "read": 128}

OTHER = {"y": "z", "z": "y"}
SIZES = {"kv": KV, "tp": TP, "y": 4, "z": 4, "x": 4, "core": 2}

F32 = jnp.float32
BF16 = jnp.bfloat16
MESH = pl.DeviceIdType.MESH


def silu(v):
    return v / (1.0 + jnp.exp(-v))


def dot(a, b):
    return jnp.dot(a, b, preferred_element_type=F32)


HOPS = (0, 1, 2, 1)
NEAR = {2: (1,), 4: (2, 1, 3), 8: (4, 5, 2, 3, 6, 7, 1)}
FARTHEST_FIRST = tuple(sorted(range(1, KV), key=lambda d: -HOPS[d // 4] - HOPS[d % 4]))


class Exchange:
    def __init__(self):
        self.kv = lax.axis_index("kv")
        self.tp = lax.axis_index("tp")
        self.at = {
            "kv": self.kv, "tp": self.tp, "z": self.kv // 4, "y": self.kv % 4, "x": self.tp // 2, "core": self.tp % 2
        }
        self.sent = []

    def peer(self, axis, d):
        z, y = self.at["z"], self.at["y"]
        if axis == "tp":
            place = (self.tp + d) % TP
            return place, (self.kv, place)
        if axis == "kv":
            place = ((z + d // 4) % 4) * 4 + (y + d % 4) % 4
            return place, (place, self.tp)
        place = (self.at[axis] + d) % SIZES[axis]
        if axis == "x":
            return place, (self.kv, place * 2 + self.at["core"])
        if axis == "core":
            return place, (self.kv, self.at["x"] * 2 + place)
        return place, (place * 4 + y if axis == "z" else z * 4 + place, self.tp)

    def each(self, axis, act):
        for d in FARTHEST_FIRST if axis == "kv" else NEAR[SIZES[axis]]:
            act(d)

    def barrier(self):
        bar = pltpu.get_barrier_semaphore()
        for axis in ("tp", "y", "z"):
            self.each(
                axis,
                lambda d: pl.semaphore_signal(
                    bar, inc=1, device_id=self.peer(axis, d)[1], device_id_type=MESH
                ),
            )
        with jax.named_scope("barrier"):
            pl.semaphore_wait(bar, TP - 1 + 3 + 3)

    def copies(self, axis, src_for, dst_for, sems):
        def act(d):
            place, device = self.peer(axis, d)
            pltpu.make_async_remote_copy(
                src_for(place), dst_for(d), sems.at[0], sems.at[1], device_id=device, device_id_type=MESH
            ).start()

        with jax.named_scope("send_" + axis):
            self.each(axis, act)

    def scatter(self, axis, src, dst, sems):
        self.copies(axis, lambda place: src.at[place], lambda d: dst.at[d - 1], sems)
        self.sent.append((dst, sems))

    def spread(self, axis, buf, sems):
        mine = buf.at[self.at[axis]]
        self.copies(axis, lambda place: mine, lambda d: mine, sems)
        self.sent.append((buf.at[pl.ds(0, SIZES[axis] - 1)], sems))

    def arrived(self, dst, sems):
        with jax.named_scope("wait"):
            pltpu.make_async_copy(dst, dst, sems.at[1]).wait()

    def arrived_all(self, buf, sems):
        self.arrived(buf.at[pl.ds(0, buf.shape[0] - 1)], sems)

    def drain(self):
        with jax.named_scope("drain"):
            for dst, sems in self.sent:
                pltpu.make_async_copy(dst, dst, sems.at[0]).wait()


def store_blocks(ref, lo, value, axis):
    size = value.shape[1]
    value = value.reshape(4, 4, 8, size).astype(BF16)
    if axis == "z":
        ref[:, :, :, lo : lo + size] = value
    else:
        for p in range(4):
            ref[p, :, :, lo : lo + size] = value[:, p]


def plus(total, recv):
    for d in range(recv.shape[0]):
        total = total + recv[d].astype(F32)
    return total


def lift(cur, gain_ref):
    wide = cur.astype(F32)
    squares = jnp.sum(wide * wide, axis=1, keepdims=True)
    lifted = (wide * gain_ref[...].reshape(1, FEAT).astype(F32)).astype(BF16)
    return lifted, squares


def half_channel(ex, cur, which, vmem, loaded, bufs, scale_ref, sem, sem_sq):
    gain, gate, up, down = (which + end for end in ("_gain", "_gate", "_up", "_down"))
    squares_bufs, bufs = bufs[:2], bufs[2:]
    count = len(CHUNKS)
    first, got, second, hid = (bufs[count * k : count * k + count] for k in range(4))
    loaded(gain)
    lifted, squares = lift(cur, vmem[gain])
    squares_bufs[0][ex.at["y"]] = jnp.transpose(jnp.broadcast_to(squares, (ROWS, 128)))[0:1]
    ex.spread("y", squares_bufs[0], sem_sq.at[0])
    loaded(gate, up)
    for i, (lo, size, axis) in enumerate(CHUNKS):
        store_blocks(first[i], 0, dot(lifted, vmem[gate][:, lo : lo + size]), axis)
        store_blocks(first[i], size, dot(lifted, vmem[up][:, lo : lo + size]), axis)
        ex.scatter(axis, first[i], got[i], sem.at[0, i])
    ex.arrived_all(squares_bufs[0], sem_sq.at[0])
    squares_bufs[1][ex.at["z"]] = jnp.sum(squares_bufs[0][...], axis=0)
    ex.spread("z", squares_bufs[1], sem_sq.at[1])
    for i, (lo, size, axis) in enumerate(CHUNKS):
        ex.arrived(got[i], sem.at[0, i])
        total = plus(first[i][ex.at[axis]].astype(F32), got[i])
        second[i][ex.at[OTHER[axis]]] = total.astype(BF16)
        ex.spread(OTHER[axis], second[i], sem.at[1, i])
    ex.arrived_all(squares_bufs[1], sem_sq.at[1])
    scale = lax.rsqrt(jnp.sum(squares_bufs[1][...], axis=0) / D + EPS)
    scale_ref[...] = jnp.transpose(jnp.broadcast_to(scale, (128, ROWS))).reshape(4, 4, 8, 128)
    scales = {"y": scale_ref[:, ex.at["y"]][:, :, 0:1], "z": scale_ref[ex.at["z"]][:, :, 0:1]}
    for i, (lo, size, axis) in enumerate(CHUNKS):
        ex.arrived_all(second[i], sem.at[1, i])
        total = plus(second[i][0].astype(F32), second[i].at[pl.ds(1, 3)])
        hidden = silu(total[:, :, :size] * scales[axis]) * (total[:, :, size:] * scales[axis])
        hid[i][ex.at[axis]] = hidden.astype(BF16)
        ex.spread(axis, hid[i], sem.at[2, i])
    loaded(down)
    part = None
    for i, (lo, size, axis) in enumerate(CHUNKS):
        ex.arrived_all(hid[i], sem.at[2, i])
        rows = hid[i][...].astype(F32)
        if axis == "y":
            rows = jnp.stack([rows[:, z] for z in range(4)], axis=0)
        p = dot(rows.reshape(ROWS, size).astype(BF16), vmem[down][lo : lo + size, :])
        part = p if part is None else part + p
    return part


def whole_sum(ex, part, cur, factor, bufs, sem):
    send, recv, mine, other = bufs
    send[...] = part.astype(BF16)
    ex.copies("x", lambda place: send, lambda d: recv.at[d - 1], sem.at[0])
    ex.sent.append((recv, sem.at[0]))
    ex.arrived(recv, sem.at[0])
    total = plus(part, recv)
    mine[...] = total
    ex.copies("core", lambda place: mine, lambda d: other, sem.at[1])
    ex.sent.append((other, sem.at[1]))
    ex.arrived(other, sem.at[1])
    return (cur.astype(F32) + factor * (total + other[...])).astype(BF16)


NAMES = (
    "block_in", "before_gain", "before_gate", "before_up", "before_down", "mix_gain", "input_gate",
    "input_value", "input_write", "input_read", "input_step", "step_bias", "decay_log", "skip_gain",
    "value_taps", "write_taps", "read_taps", "value_window", "write_window", "read_window", "scan_state",
    "group_gain", "mixer_out", "after_gain", "after_gate", "after_up", "after_down",
)


def kernel(
    *refs,
):
    count = len(NAMES)
    hbm = dict(zip(NAMES, refs[:count]))
    block_out, state_out, value_next, write_next, read_next = refs[count : count + 5]
    vmem = dict(zip(NAMES, refs[count + 5 : 2 * count + 5]))
    load_sem, *rest = refs[2 * count + 5 :]

    def take(count):
        taken = rest[:count]
        del rest[:count]
        return taken

    packed, scale_ref, olds = take(3)
    a_bufs, b_bufs = take(2 + 4 * len(CHUNKS)), take(2 + 4 * len(CHUNKS))
    tile_send, tile_recv = take(2)
    m_bufs, m_hid = [[take(4) for chunk in MIXED] for g in range(2)], take(2)
    t1_bufs, t2_bufs = take(4), take(4)
    t3_own, t3_send, t3_recv = take(3)
    sem_in, sem_a, sem_b, sem_a_sq, sem_b_sq, sem_m, sem_tile, sem_hid, sem_t1, sem_t2, sem_t3 = take(11)
    ex = Exchange()
    loads = {n: pltpu.make_async_copy(hbm[n], vmem[n], load_sem.at[i]) for i, n in enumerate(NAMES) if n != "block_in"}
    mine = pltpu.make_async_copy(hbm["block_in"], packed.at[ex.tp], load_sem.at[0])
    mine.start()
    for copy in loads.values():
        copy.start()

    def loaded(*names):
        with jax.named_scope("loaded"):
            for n in names:
                loads[n].wait()

    ex.barrier()
    mine.wait()
    ex.spread("tp", packed, sem_in)
    ex.arrived_all(packed, sem_in)
    cur = jnp.transpose(packed[...].astype(F32).reshape(FEAT, ROWS)).astype(BF16)

    part = half_channel(ex, cur, "before", vmem, loaded, a_bufs, scale_ref, sem_a, sem_a_sq)
    cur = whole_sum(ex, part, cur, 0.5, t1_bufs, sem_t1)

    loaded("mix_gain", "input_gate", "input_value", "input_write", "input_read", "input_step")
    lifted, squares = lift(cur, vmem["mix_gain"])
    lanes = [slice(GROUP * g, GROUP * g + GROUP) for g in range(2)]
    states = [slice(STATE * g, STATE * g + STATE) for g in range(2)]
    for g in range(2):
        for k, (axis, pieces) in enumerate(MIXED):
            first, got = m_bufs[g][k][:2]
            at = 0
            for kind, lo, size in pieces:
                lo += WIDTHS[kind] * g
                store_blocks(first, at, dot(lifted, vmem["input_" + kind][:, lo : lo + size]), axis)
                at += size
            ex.scatter(axis, first, got, sem_m.at[g, k, 0])
        if g == 0:
            place = lax.broadcasted_iota(jnp.int32, (128, HEADS), 0)
            head = lax.broadcasted_iota(jnp.int32, (128, HEADS), 1)
            spots = jnp.where(place == head, 1.0, 0.0).astype(BF16)
            step_w = dot(spots, vmem["input_step"][...]).astype(BF16)
            step = lax.dot_general(lifted, step_w, (((1,), (1,)), ((), ())), preferred_element_type=F32)
            lane = lax.broadcasted_iota(jnp.int32, (ROWS, 128), 1)
            tile_send[...] = jnp.where(lane < HEADS, step, squares).reshape(KV, 8, 128)
            ex.scatter("kv", tile_send, tile_recv, sem_tile)
    loaded("step_bias", "decay_log", "skip_gain", "group_gain", "scan_state")
    with jax.named_scope("olds"):
        for g in range(2):
            for r in range(8):
                old = vmem["scan_state"][r, 8 * g : 8 * g + 8].reshape(GROUP, STATE)
                olds[g, :, STATE * r : STATE * r + STATE] = old.astype(BF16)
    loaded(*(a + b for a in ("value", "write", "read") for b in ("_taps", "_window")))
    for g in range(2):
        for k, (axis, _) in enumerate(MIXED):
            first, got, second, last = m_bufs[g][k]
            ex.arrived(got, sem_m.at[g, k, 0])
            second[...] = plus(first[ex.at[axis]].astype(F32), got).astype(BF16)
            ex.scatter(OTHER[axis], second, last, sem_m.at[g, k, 1])

    ex.arrived(tile_recv, sem_tile)
    tile = plus(tile_send[ex.kv], tile_recv)
    scale = lax.rsqrt(tile[:, HEADS : HEADS + 1] / D + EPS)
    raw = tile[:, :HEADS] * scale + vmem["step_bias"][...].reshape(1, HEADS)
    step_size = jnp.maximum(raw, 0.0) + jnp.log1p(jnp.exp(-jnp.abs(raw)))
    decay = jnp.exp(-step_size * jnp.exp(vmem["decay_log"][...].reshape(1, HEADS)))
    skip = jnp.broadcast_to(vmem["skip_gain"][...].reshape(1, HEADS), (8, HEADS))
    of = lax.broadcasted_iota(jnp.int32, (HEADS, INNER), 1) // HEAD_DIM
    row = lax.broadcasted_iota(jnp.int32, (HEADS, INNER), 0)
    heads = jnp.dot(
        jnp.concatenate([step_size, decay, skip], axis=0),
        jnp.where(of == row, 1.0, 0.0),
        preferred_element_type=F32,
        precision=lax.Precision.HIGHEST,
    )
    gain = vmem["group_gain"][...].reshape(1, INNER).astype(F32)
    updates = []
    for g in range(2):
        sums = {kind: [] for kind in WIDTHS}
        for k, (axis, pieces) in enumerate(MIXED):
            first, got, second, last = m_bufs[g][k]
            ex.arrived(last, sem_m.at[g, k, 1])
            total = plus(second[ex.at[OTHER[axis]]].astype(F32), last) * scale
            at = 0
            for kind, lo, size in pieces:
                sums[kind].append(total[:, at : at + size])
                at += size
        sums = {kind: jnp.concatenate(found, axis=1) for kind, found in sums.items()}
        next_refs = {"value": value_next, "write": write_next, "read": read_next}

        def conv(fresh, kind, at):
            window = [vmem[kind + "_window"][i, :, at] for i in range(3)] + [fresh.astype(BF16)]
            taps = vmem[kind + "_taps"][:, at].astype(F32)
            acc = None
            for i in range(4):
                if i:
                    next_refs[kind][i - 1, :, at] = window[i]
                term = window[i].astype(F32) * taps[i : i + 1]
                acc = term if acc is None else acc + term
            return silu(acc)

        gate_rows = sums["gate"].astype(BF16).astype(F32)
        write = conv(sums["write"], "write", states[g])
        value = conv(sums["value"], "value", lanes[g])
        read = conv(sums["read"], "read", states[g])
        step_x = heads[0:8, lanes[g]] * value
        row = lax.broadcasted_iota(jnp.int32, (8, STATE), 0)
        reads = jnp.concatenate([jnp.where(row == r, read, 0.0) for r in range(8)], axis=1).astype(BF16)
        kept = lax.dot_general(reads, olds[g], (((1,), (1,)), ((), ())), preferred_element_type=F32)
        meet = jnp.sum(write * read, axis=1, keepdims=True)
        readout = heads[8:16, lanes[g]] * kept + step_x * meet + heads[16:24, lanes[g]] * value
        gated = readout * silu(gate_rows)
        mean = jnp.sum(gated * gated, axis=1, keepdims=True) / GROUP
        m_hid[g][ex.kv] = (gated * lax.rsqrt(mean + EPS) * gain[:, lanes[g]]).astype(BF16)
        ex.spread("kv", m_hid[g], sem_hid.at[g])
        updates.append((step_x, heads[8:16, lanes[g]], write))
    with jax.named_scope("update"):
        for g, (step_x, kept, write) in enumerate(updates):
            across = jnp.transpose(jnp.concatenate([step_x, kept], axis=0))
            for r in range(8):
                old = vmem["scan_state"][r, 8 * g : 8 * g + 8].reshape(GROUP, STATE)
                new = across[:, 8 + r : 9 + r] * old + across[:, r : r + 1] * write[r : r + 1]
                state_out[r, 8 * g : 8 * g + 8] = new.reshape(8, HEAD_DIM, STATE)
    loaded("mixer_out")
    part = None
    for g in range(2):
        ex.arrived_all(m_hid[g], sem_hid.at[g])
        rows = m_hid[g][...].astype(F32).reshape(ROWS, GROUP).astype(BF16)
        p = dot(rows, vmem["mixer_out"][lanes[g], :])
        part = p if part is None else part + p
    cur = whole_sum(ex, part, cur, 1.0, t2_bufs, sem_t2)

    part = half_channel(ex, cur, "after", vmem, loaded, b_bufs, scale_ref, sem_b, sem_b_sq)
    columns = jnp.transpose(part).reshape(TP, 32, ROWS)
    t3_own[...] = columns
    t3_send[...] = columns.astype(BF16)
    ex.scatter("tp", t3_send, t3_recv, sem_t3)
    total = t3_own[ex.tp]
    t3_own[...] = jnp.transpose(cur.astype(F32)).reshape(TP, 32, ROWS)
    ex.arrived(t3_recv, sem_t3)
    total = plus(total, t3_recv)
    block_out[...] = (t3_own[ex.tp] + 0.5 * total).astype(BF16)
    ex.drain()


def store(*refs):
    srcs, dsts, sem = refs[: (len(refs) - 1) // 2], refs[(len(refs) - 1) // 2 : -1], refs[-1]
    copies = [pltpu.make_async_copy(s, d, sem.at[i]) for i, (s, d) in enumerate(zip(srcs, dsts))]
    for copy in copies:
        copy.start()
    for copy in copies:
        copy.wait()


def local(*args):
    named = dict(zip(NAMES, args))
    named["block_in"] = named["block_in"].T
    named["input_step"] = named["input_step"].T
    for kind in ("value", "write", "read"):
        named[kind + "_window"] = named[kind + "_window"].transpose(1, 0, 2)
    operands = [pltpu.with_memory_space_constraint(named[n], pltpu.HBM) for n in NAMES]
    vmem = pl.BlockSpec(memory_space=pltpu.VMEM)
    hbm = pl.BlockSpec(memory_space=pltpu.HBM)

    def v(*shape, dtype=BF16):
        return pltpu.VMEM(shape, dtype)

    def parts(lead, scale, chunks):
        return [v(*lead, 8, scale * size) for _, size, _ in chunks]

    channel = [
        v(4, 1, ROWS, dtype=F32), v(4, 1, ROWS, dtype=F32),
        *parts((4, 4), 2, CHUNKS), *parts((3, 4), 2, CHUNKS), *parts((4, 4), 2, CHUNKS), *parts((4, 4), 1, CHUNKS),
    ]
    tp_sum = [v(ROWS, FEAT), v(3, ROWS, FEAT), v(ROWS, FEAT, dtype=F32), v(ROWS, FEAT, dtype=F32)]
    mixer = []
    for _, pieces in 2 * MIXED:
        width = sum(size for _, _, size in pieces)
        mixer += [v(4, 4, 8, width), v(3, 4, 8, width), v(4, 8, width), v(3, 8, width)]
    mixer += 2 * [v(KV, 8, GROUP)]
    sems = pltpu.SemaphoreType.DMA
    shapes = (
        jax.ShapeDtypeStruct((32, ROWS), BF16),
        jax.ShapeDtypeStruct(named["scan_state"].shape, F32),
        jax.ShapeDtypeStruct((3, 8, INNER), BF16),
        jax.ShapeDtypeStruct((3, 8, 256), BF16),
        jax.ShapeDtypeStruct((3, 8, 256), BF16),
    )
    results = pl.pallas_call(
        kernel,
        out_shape=shapes,
        in_specs=[hbm] * len(operands),
        out_specs=(vmem,) * 5,
        scratch_shapes=[
            *[v(*a.shape, dtype=a.dtype) for a in operands],
            sems((len(NAMES),)),
            v(TP, 32, 128), v(4, 4, 8, 128, dtype=F32), v(2, GROUP, 8 * STATE),
            *channel, *channel,
            v(KV, 8, 128, dtype=F32), v(KV - 1, 8, 128, dtype=F32), *mixer,
            *tp_sum, *tp_sum,
            v(TP, 32, 128, dtype=F32), v(TP, 32, 128), v(TP - 1, 32, 128),
            sems((2,)), sems((3, len(CHUNKS), 2)), sems((3, len(CHUNKS), 2)), sems((2, 2)), sems((2, 2)),
            sems((2, len(MIXED), 2, 2)), sems((2,)), sems((2, 2)), sems((2, 2)), sems((2, 2)), sems((2,)),
        ],
        compiler_params=pltpu.CompilerParams(
            collective_id=0, has_side_effects=True, vmem_limit_bytes=40 * 1024 * 1024
        ),
        name="layer",
    )(*operands)
    block_out, state_next, *windows = pl.pallas_call(
        store,
        out_shape=shapes,
        in_specs=[vmem] * 5,
        out_specs=(hbm,) * 5,
        scratch_shapes=[sems((5,))],
        compiler_params=pltpu.CompilerParams(vmem_limit_bytes=4 * 1024 * 1024),
        name="store",
    )(*results)
    return (block_out.T, state_next, *[w.transpose(1, 0, 2) for w in windows])


def solution(mesh):
    placed = (
        P(None, ("kv", "tp")),
        P("kv"),
        P("kv", "tp"),
        P("kv", "tp"),
        P("tp", "kv"),
        P("kv"),
        P("kv", "tp"),
        P("kv", "tp"),
        P("kv", "tp"),
        P("kv", "tp"),
        P("kv", "tp"),
        P("tp"),
        P("tp"),
        P("tp"),
        P(None, "tp"),
        P(None, "tp"),
        P(None, "tp"),
        P("kv", None, "tp"),
        P("kv", None, "tp"),
        P("kv", None, "tp"),
        P("kv", "tp", None, None),
        P("tp"),
        P("tp", "kv"),
        P("kv"),
        P("kv", "tp"),
        P("kv", "tp"),
        P("tp", "kv"),
    )
    return jax.shard_map(
        local,
        mesh=mesh,
        in_specs=placed,
        out_specs=(
            P(None, ("kv", "tp")),
            P("kv", "tp", None, None),
            P("kv", None, "tp"),
            P("kv", None, "tp"),
            P("kv", None, "tp"),
        ),
        check_vma=False,
    )
```

```python
import jax
import jax.numpy as jnp
from jax import lax
from jax.experimental import pallas as pl
from jax.experimental.pallas import tpu as pltpu
from jax.sharding import PartitionSpec as P

D = 4096
HEAD_DIM = 64
STATE = 128
EPS = 1e-06

KV = 16
TP = 8
ROWS = 128
FEAT = 256
HID = 1408
INNER = 1024
HEADS = 16
CHUNKS = ((0, 128, "y"), (128, 128, "z"), (256, 128, "y"), (384, 128, "z"), (512, 128, "y"), (640, 128, "z"), (768, 128, "y"), (896, 128, "z"), (1024, 128, "y"), (1152, 128, "z"), (1280, 128, "y"))
GROUP = 512
MIXED = (
    ("y", (("gate", 0, 512), ("write", 0, 128))),
    ("z", (("value", 0, 512), ("read", 0, 128))),
)
WIDTHS = {"gate": 512, "value": 512, "write": 128, "read": 128}

OTHER = {"y": "z", "z": "y"}
SIZES = {"kv": KV, "tp": TP, "y": 4, "z": 4, "x": 4, "core": 2}

F32 = jnp.float32
BF16 = jnp.bfloat16
MESH = pl.DeviceIdType.MESH


def silu(v):
    return v / (1.0 + jnp.exp(-v))


def dot(a, b):
    return jnp.dot(a, b, preferred_element_type=F32)


HOPS = (0, 1, 2, 1)
NEAR = {2: (1,), 4: (2, 1, 3), 8: (4, 5, 2, 3, 6, 7, 1)}
FARTHEST_FIRST = tuple(sorted(range(1, KV), key=lambda d: -HOPS[d // 4] - HOPS[d % 4]))


class Exchange:
    def __init__(self):
        self.kv = lax.axis_index("kv")
        self.tp = lax.axis_index("tp")
        self.at = {
            "kv": self.kv, "tp": self.tp, "z": self.kv // 4, "y": self.kv % 4, "x": self.tp // 2, "core": self.tp % 2
        }
        self.sent = []

    def peer(self, axis, d):
        z, y = self.at["z"], self.at["y"]
        if axis == "tp":
            place = (self.tp + d) % TP
            return place, (self.kv, place)
        if axis == "kv":
            place = ((z + d // 4) % 4) * 4 + (y + d % 4) % 4
            return place, (place, self.tp)
        place = (self.at[axis] + d) % SIZES[axis]
        if axis == "x":
            return place, (self.kv, place * 2 + self.at["core"])
        if axis == "core":
            return place, (self.kv, self.at["x"] * 2 + place)
        return place, (place * 4 + y if axis == "z" else z * 4 + place, self.tp)

    def each(self, axis, act):
        for d in FARTHEST_FIRST if axis == "kv" else NEAR[SIZES[axis]]:
            act(d)

    def barrier(self):
        bar = pltpu.get_barrier_semaphore()
        for axis in ("tp", "y", "z"):
            self.each(
                axis,
                lambda d: pl.semaphore_signal(
                    bar, inc=1, device_id=self.peer(axis, d)[1], device_id_type=MESH
                ),
            )
        with jax.named_scope("barrier"):
            pl.semaphore_wait(bar, TP - 1 + 3 + 3)

    def copies(self, axis, src_for, dst_for, sems):
        def act(d):
            place, device = self.peer(axis, d)
            pltpu.make_async_remote_copy(
                src_for(place), dst_for(d), sems.at[0], sems.at[1], device_id=device, device_id_type=MESH
            ).start()

        with jax.named_scope("send_" + axis):
            self.each(axis, act)

    def scatter(self, axis, src, dst, sems):
        self.copies(axis, lambda place: src.at[place], lambda d: dst.at[d - 1], sems)
        self.sent.append((dst, sems))

    def spread(self, axis, buf, sems):
        mine = buf.at[self.at[axis]]
        self.copies(axis, lambda place: mine, lambda d: mine, sems)
        self.sent.append((buf.at[pl.ds(0, SIZES[axis] - 1)], sems))

    def arrived(self, dst, sems):
        with jax.named_scope("wait"):
            pltpu.make_async_copy(dst, dst, sems.at[1]).wait()

    def arrived_all(self, buf, sems):
        self.arrived(buf.at[pl.ds(0, buf.shape[0] - 1)], sems)

    def drain(self):
        with jax.named_scope("drain"):
            for dst, sems in self.sent:
                pltpu.make_async_copy(dst, dst, sems.at[0]).wait()


def store_blocks(ref, lo, value, axis):
    size = value.shape[1]
    value = value.reshape(4, 4, 8, size).astype(BF16)
    if axis == "z":
        ref[:, :, :, lo : lo + size] = value
    else:
        for p in range(4):
            ref[p, :, :, lo : lo + size] = value[:, p]


def plus(total, recv):
    for d in range(recv.shape[0]):
        total = total + recv[d].astype(F32)
    return total


def lift(cur, gain_ref):
    wide = cur.astype(F32)
    squares = jnp.sum(wide * wide, axis=1, keepdims=True)
    lifted = (wide * gain_ref[...].reshape(1, FEAT).astype(F32)).astype(BF16)
    return lifted, squares


def half_channel(ex, cur, which, vmem, loaded, bufs, scale_ref, sem, sem_sq):
    gain, gate, up, down = (which + end for end in ("_gain", "_gate", "_up", "_down"))
    squares_bufs, bufs = bufs[:2], bufs[2:]
    count = len(CHUNKS)
    first, got, second, hid = (bufs[count * k : count * k + count] for k in range(4))
    loaded(gain)
    lifted, squares = lift(cur, vmem[gain])
    squares_bufs[0][ex.at["y"]] = jnp.transpose(jnp.broadcast_to(squares, (ROWS, 128)))[0:1]
    ex.spread("y", squares_bufs[0], sem_sq.at[0])
    loaded(gate, up)
    for i, (lo, size, axis) in enumerate(CHUNKS):
        store_blocks(first[i], 0, dot(lifted, vmem[gate][:, lo : lo + size]), axis)
        store_blocks(first[i], size, dot(lifted, vmem[up][:, lo : lo + size]), axis)
        ex.scatter(axis, first[i], got[i], sem.at[0, i])
    ex.arrived_all(squares_bufs[0], sem_sq.at[0])
    squares_bufs[1][ex.at["z"]] = jnp.sum(squares_bufs[0][...], axis=0)
    ex.spread("z", squares_bufs[1], sem_sq.at[1])
    for i, (lo, size, axis) in enumerate(CHUNKS):
        ex.arrived(got[i], sem.at[0, i])
        total = plus(first[i][ex.at[axis]].astype(F32), got[i])
        second[i][ex.at[OTHER[axis]]] = total.astype(BF16)
        ex.spread(OTHER[axis], second[i], sem.at[1, i])
    ex.arrived_all(squares_bufs[1], sem_sq.at[1])
    scale = lax.rsqrt(jnp.sum(squares_bufs[1][...], axis=0) / D + EPS)
    scale_ref[...] = jnp.transpose(jnp.broadcast_to(scale, (128, ROWS))).reshape(4, 4, 8, 128)
    scales = {"y": scale_ref[:, ex.at["y"]][:, :, 0:1], "z": scale_ref[ex.at["z"]][:, :, 0:1]}
    for i, (lo, size, axis) in enumerate(CHUNKS):
        ex.arrived_all(second[i], sem.at[1, i])
        total = plus(second[i][0].astype(F32), second[i].at[pl.ds(1, 3)])
        hidden = silu(total[:, :, :size] * scales[axis]) * (total[:, :, size:] * scales[axis])
        hid[i][ex.at[axis]] = hidden.astype(BF16)
        ex.spread(axis, hid[i], sem.at[2, i])
    loaded(down)
    part = None
    for i, (lo, size, axis) in enumerate(CHUNKS):
        ex.arrived_all(hid[i], sem.at[2, i])
        rows = hid[i][...].astype(F32)
        if axis == "y":
            rows = jnp.stack([rows[:, z] for z in range(4)], axis=0)
        p = dot(rows.reshape(ROWS, size).astype(BF16), vmem[down][lo : lo + size, :])
        part = p if part is None else part + p
    return part


def whole_sum(ex, part, cur, factor, bufs, sem):
    send, recv, mine, other = bufs
    send[...] = part.astype(BF16)
    ex.copies("x", lambda place: send, lambda d: recv.at[d - 1], sem.at[0])
    ex.sent.append((recv, sem.at[0]))
    ex.arrived(recv, sem.at[0])
    total = plus(part, recv)
    mine[...] = total.astype(BF16)
    ex.copies("core", lambda place: mine, lambda d: other, sem.at[1])
    ex.sent.append((other, sem.at[1]))
    ex.arrived(other, sem.at[1])
    return (cur.astype(F32) + factor * (total + other[...].astype(F32))).astype(BF16)


NAMES = (
    "block_in", "before_gain", "before_gate", "before_up", "before_down", "mix_gain", "input_gate",
    "input_value", "input_write", "input_read", "input_step", "step_bias", "decay_log", "skip_gain",
    "value_taps", "write_taps", "read_taps", "value_window", "write_window", "read_window", "scan_state",
    "group_gain", "mixer_out", "after_gain", "after_gate", "after_up", "after_down",
)


def kernel(
    *refs,
):
    count = len(NAMES)
    hbm = dict(zip(NAMES, refs[:count]))
    block_out, state_out, value_next, write_next, read_next = refs[count : count + 5]
    vmem = dict(zip(NAMES, refs[count + 5 : 2 * count + 5]))
    load_sem, *rest = refs[2 * count + 5 :]

    def take(count):
        taken = rest[:count]
        del rest[:count]
        return taken

    packed, scale_ref, olds = take(3)
    a_bufs, b_bufs = take(2 + 4 * len(CHUNKS)), take(2 + 4 * len(CHUNKS))
    tile_send, tile_recv = take(2)
    m_bufs, m_hid = [[take(4) for chunk in MIXED] for g in range(2)], take(2)
    t1_bufs, t2_bufs = take(4), take(4)
    t3_own, t3_send, t3_recv = take(3)
    sem_in, sem_a, sem_b, sem_a_sq, sem_b_sq, sem_m, sem_tile, sem_hid, sem_t1, sem_t2, sem_t3 = take(11)
    ex = Exchange()
    loads = {n: pltpu.make_async_copy(hbm[n], vmem[n], load_sem.at[i]) for i, n in enumerate(NAMES) if n != "block_in"}
    mine = pltpu.make_async_copy(hbm["block_in"], packed.at[ex.tp], load_sem.at[0])
    mine.start()
    for copy in loads.values():
        copy.start()

    def loaded(*names):
        with jax.named_scope("loaded"):
            for n in names:
                loads[n].wait()

    ex.barrier()
    mine.wait()
    ex.spread("tp", packed, sem_in)
    ex.arrived_all(packed, sem_in)
    cur = jnp.transpose(packed[...].astype(F32).reshape(FEAT, ROWS)).astype(BF16)

    part = half_channel(ex, cur, "before", vmem, loaded, a_bufs, scale_ref, sem_a, sem_a_sq)
    cur = whole_sum(ex, part, cur, 0.5, t1_bufs, sem_t1)

    loaded("mix_gain", "input_gate", "input_value", "input_write", "input_read", "input_step")
    lifted, squares = lift(cur, vmem["mix_gain"])
    lanes = [slice(GROUP * g, GROUP * g + GROUP) for g in range(2)]
    states = [slice(STATE * g, STATE * g + STATE) for g in range(2)]
    for g in range(2):
        for k, (axis, pieces) in enumerate(MIXED):
            first, got = m_bufs[g][k][:2]
            at = 0
            for kind, lo, size in pieces:
                lo += WIDTHS[kind] * g
                store_blocks(first, at, dot(lifted, vmem["input_" + kind][:, lo : lo + size]), axis)
                at += size
            ex.scatter(axis, first, got, sem_m.at[g, k, 0])
        if g == 0:
            place = lax.broadcasted_iota(jnp.int32, (128, HEADS), 0)
            head = lax.broadcasted_iota(jnp.int32, (128, HEADS), 1)
            spots = jnp.where(place == head, 1.0, 0.0).astype(BF16)
            step_w = dot(spots, vmem["input_step"][...]).astype(BF16)
            step = lax.dot_general(lifted, step_w, (((1,), (1,)), ((), ())), preferred_element_type=F32)
            lane = lax.broadcasted_iota(jnp.int32, (ROWS, 128), 1)
            tile_send[...] = jnp.where(lane < HEADS, step, squares).reshape(KV, 8, 128)
            ex.scatter("kv", tile_send, tile_recv, sem_tile)
    loaded("step_bias", "decay_log", "skip_gain", "group_gain", "scan_state")
    with jax.named_scope("olds"):
        for g in range(2):
            for r in range(8):
                old = vmem["scan_state"][r, 8 * g : 8 * g + 8].reshape(GROUP, STATE)
                olds[g, :, STATE * r : STATE * r + STATE] = old.astype(BF16)
    loaded(*(a + b for a in ("value", "write", "read") for b in ("_taps", "_window")))
    for g in range(2):
        for k, (axis, _) in enumerate(MIXED):
            first, got, second, last = m_bufs[g][k]
            ex.arrived(got, sem_m.at[g, k, 0])
            second[...] = plus(first[ex.at[axis]].astype(F32), got).astype(BF16)
            ex.scatter(OTHER[axis], second, last, sem_m.at[g, k, 1])

    ex.arrived(tile_recv, sem_tile)
    tile = plus(tile_send[ex.kv], tile_recv)
    scale = lax.rsqrt(tile[:, HEADS : HEADS + 1] / D + EPS)
    raw = tile[:, :HEADS] * scale + vmem["step_bias"][...].reshape(1, HEADS)
    step_size = jnp.maximum(raw, 0.0) + jnp.log1p(jnp.exp(-jnp.abs(raw)))
    decay = jnp.exp(-step_size * jnp.exp(vmem["decay_log"][...].reshape(1, HEADS)))
    skip = jnp.broadcast_to(vmem["skip_gain"][...].reshape(1, HEADS), (8, HEADS))
    of = lax.broadcasted_iota(jnp.int32, (HEADS, INNER), 1) // HEAD_DIM
    row = lax.broadcasted_iota(jnp.int32, (HEADS, INNER), 0)
    heads = jnp.dot(
        jnp.concatenate([step_size, decay, skip], axis=0),
        jnp.where(of == row, 1.0, 0.0),
        preferred_element_type=F32,
        precision=lax.Precision.HIGHEST,
    )
    gain = vmem["group_gain"][...].reshape(1, INNER).astype(F32)
    updates = []
    for g in range(2):
        sums = {kind: [] for kind in WIDTHS}
        for k, (axis, pieces) in enumerate(MIXED):
            first, got, second, last = m_bufs[g][k]
            ex.arrived(last, sem_m.at[g, k, 1])
            total = plus(second[ex.at[OTHER[axis]]].astype(F32), last) * scale
            at = 0
            for kind, lo, size in pieces:
                sums[kind].append(total[:, at : at + size])
                at += size
        sums = {kind: jnp.concatenate(found, axis=1) for kind, found in sums.items()}
        next_refs = {"value": value_next, "write": write_next, "read": read_next}

        def conv(fresh, kind, at):
            window = [vmem[kind + "_window"][i, :, at] for i in range(3)] + [fresh.astype(BF16)]
            taps = vmem[kind + "_taps"][:, at].astype(F32)
            acc = None
            for i in range(4):
                if i:
                    next_refs[kind][i - 1, :, at] = window[i]
                term = window[i].astype(F32) * taps[i : i + 1]
                acc = term if acc is None else acc + term
            return silu(acc)

        gate_rows = sums["gate"].astype(BF16).astype(F32)
        write = conv(sums["write"], "write", states[g])
        value = conv(sums["value"], "value", lanes[g])
        read = conv(sums["read"], "read", states[g])
        step_x = heads[0:8, lanes[g]] * value
        row = lax.broadcasted_iota(jnp.int32, (8, STATE), 0)
        reads = jnp.concatenate([jnp.where(row == r, read, 0.0) for r in range(8)], axis=1).astype(BF16)
        kept = lax.dot_general(reads, olds[g], (((1,), (1,)), ((), ())), preferred_element_type=F32)
        meet = jnp.sum(write * read, axis=1, keepdims=True)
        readout = heads[8:16, lanes[g]] * kept + step_x * meet + heads[16:24, lanes[g]] * value
        gated = readout * silu(gate_rows)
        mean = jnp.sum(gated * gated, axis=1, keepdims=True) / GROUP
        m_hid[g][ex.kv] = (gated * lax.rsqrt(mean + EPS) * gain[:, lanes[g]]).astype(BF16)
        ex.spread("kv", m_hid[g], sem_hid.at[g])
        updates.append((step_x, heads[8:16, lanes[g]], write))
    with jax.named_scope("update"):
        for g, (step_x, kept, write) in enumerate(updates):
            across = jnp.transpose(jnp.concatenate([step_x, kept], axis=0))
            for r in range(8):
                old = vmem["scan_state"][r, 8 * g : 8 * g + 8].reshape(GROUP, STATE)
                new = across[:, 8 + r : 9 + r] * old + across[:, r : r + 1] * write[r : r + 1]
                state_out[r, 8 * g : 8 * g + 8] = new.reshape(8, HEAD_DIM, STATE)
    loaded("mixer_out")
    part = None
    for g in range(2):
        ex.arrived_all(m_hid[g], sem_hid.at[g])
        rows = m_hid[g][...].astype(F32).reshape(ROWS, GROUP).astype(BF16)
        p = dot(rows, vmem["mixer_out"][lanes[g], :])
        part = p if part is None else part + p
    cur = whole_sum(ex, part, cur, 1.0, t2_bufs, sem_t2)

    part = half_channel(ex, cur, "after", vmem, loaded, b_bufs, scale_ref, sem_b, sem_b_sq)
    columns = jnp.transpose(part).reshape(TP, 32, ROWS)
    t3_own[...] = columns
    t3_send[...] = columns.astype(BF16)
    ex.scatter("tp", t3_send, t3_recv, sem_t3)
    total = t3_own[ex.tp]
    t3_own[...] = jnp.transpose(cur.astype(F32)).reshape(TP, 32, ROWS)
    ex.arrived(t3_recv, sem_t3)
    total = plus(total, t3_recv)
    block_out[...] = (t3_own[ex.tp] + 0.5 * total).astype(BF16)
    ex.drain()


def store(*refs):
    srcs, dsts, sem = refs[: (len(refs) - 1) // 2], refs[(len(refs) - 1) // 2 : -1], refs[-1]
    copies = [pltpu.make_async_copy(s, d, sem.at[i]) for i, (s, d) in enumerate(zip(srcs, dsts))]
    for copy in copies:
        copy.start()
    for copy in copies:
        copy.wait()


def local(*args):
    named = dict(zip(NAMES, args))
    named["block_in"] = named["block_in"].T
    named["input_step"] = named["input_step"].T
    for kind in ("value", "write", "read"):
        named[kind + "_window"] = named[kind + "_window"].transpose(1, 0, 2)
    operands = [pltpu.with_memory_space_constraint(named[n], pltpu.HBM) for n in NAMES]
    vmem = pl.BlockSpec(memory_space=pltpu.VMEM)
    hbm = pl.BlockSpec(memory_space=pltpu.HBM)

    def v(*shape, dtype=BF16):
        return pltpu.VMEM(shape, dtype)

    def parts(lead, scale, chunks):
        return [v(*lead, 8, scale * size) for _, size, _ in chunks]

    channel = [
        v(4, 1, ROWS, dtype=F32), v(4, 1, ROWS, dtype=F32),
        *parts((4, 4), 2, CHUNKS), *parts((3, 4), 2, CHUNKS), *parts((4, 4), 2, CHUNKS), *parts((4, 4), 1, CHUNKS),
    ]
    tp_sum = [v(ROWS, FEAT), v(3, ROWS, FEAT), v(ROWS, FEAT), v(ROWS, FEAT)]
    mixer = []
    for _, pieces in 2 * MIXED:
        width = sum(size for _, _, size in pieces)
        mixer += [v(4, 4, 8, width), v(3, 4, 8, width), v(4, 8, width), v(3, 8, width)]
    mixer += 2 * [v(KV, 8, GROUP)]
    sems = pltpu.SemaphoreType.DMA
    shapes = (
        jax.ShapeDtypeStruct((32, ROWS), BF16),
        jax.ShapeDtypeStruct(named["scan_state"].shape, F32),
        jax.ShapeDtypeStruct((3, 8, INNER), BF16),
        jax.ShapeDtypeStruct((3, 8, 256), BF16),
        jax.ShapeDtypeStruct((3, 8, 256), BF16),
    )
    results = pl.pallas_call(
        kernel,
        out_shape=shapes,
        in_specs=[hbm] * len(operands),
        out_specs=(vmem,) * 5,
        scratch_shapes=[
            *[v(*a.shape, dtype=a.dtype) for a in operands],
            sems((len(NAMES),)),
            v(TP, 32, 128), v(4, 4, 8, 128, dtype=F32), v(2, GROUP, 8 * STATE),
            *channel, *channel,
            v(KV, 8, 128, dtype=F32), v(KV - 1, 8, 128, dtype=F32), *mixer,
            *tp_sum, *tp_sum,
            v(TP, 32, 128, dtype=F32), v(TP, 32, 128), v(TP - 1, 32, 128),
            sems((2,)), sems((3, len(CHUNKS), 2)), sems((3, len(CHUNKS), 2)), sems((2, 2)), sems((2, 2)),
            sems((2, len(MIXED), 2, 2)), sems((2,)), sems((2, 2)), sems((2, 2)), sems((2, 2)), sems((2,)),
        ],
        compiler_params=pltpu.CompilerParams(
            collective_id=0, has_side_effects=True, vmem_limit_bytes=40 * 1024 * 1024
        ),
        name="layer",
    )(*operands)
    block_out, state_next, *windows = pl.pallas_call(
        store,
        out_shape=shapes,
        in_specs=[vmem] * 5,
        out_specs=(hbm,) * 5,
        scratch_shapes=[sems((5,))],
        compiler_params=pltpu.CompilerParams(vmem_limit_bytes=4 * 1024 * 1024),
        name="store",
    )(*results)
    return (block_out.T, state_next, *[w.transpose(1, 0, 2) for w in windows])


def solution(mesh):
    placed = (
        P(None, ("kv", "tp")),
        P("kv"),
        P("kv", "tp"),
        P("kv", "tp"),
        P("tp", "kv"),
        P("kv"),
        P("kv", "tp"),
        P("kv", "tp"),
        P("kv", "tp"),
        P("kv", "tp"),
        P("kv", "tp"),
        P("tp"),
        P("tp"),
        P("tp"),
        P(None, "tp"),
        P(None, "tp"),
        P(None, "tp"),
        P("kv", None, "tp"),
        P("kv", None, "tp"),
        P("kv", None, "tp"),
        P("kv", "tp", None, None),
        P("tp"),
        P("tp", "kv"),
        P("kv"),
        P("kv", "tp"),
        P("kv", "tp"),
        P("tp", "kv"),
    )
    return jax.shard_map(
        local,
        mesh=mesh,
        in_specs=placed,
        out_specs=(
            P(None, ("kv", "tp")),
            P("kv", "tp", None, None),
            P("kv", None, "tp"),
            P("kv", None, "tp"),
            P("kv", None, "tp"),
        ),
        check_vma=False,
    )
```
